32 devices in a mesh: sp: 8 (over z, x), tp: 4 (over y, core).
Axes of the slice: x: 2, y: 2, z: 4, core: 2. Of those that a mesh axis runs over, the one named last changes fastest.
Arguments:
- resid: bfloat16 [4096, 2048], P(('sp', 'tp')), may hold values from -6 to 6
- recurrent_input: bfloat16 [4096, 2048], P('sp', 'tp'), may hold values from -12.2 to 12.2
- recurrent_out_gate: bfloat16 [4096, 2048], P('sp', 'tp'), may hold values from -6 to 6
- filter_weight: float32 [4, 2048], P(None, 'tp'), may hold values from -3 to 3
- recurrence_gate_matrix: bfloat16 [32, 64, 64], P('tp'), may hold values from -0.75 to 0.75
- input_gate_matrix: bfloat16 [32, 64, 64], P('tp'), may hold values from -0.75 to 0.75
- channel_decay_raw: float32 [2048], P('tp'), may hold values from 4.8 to 13.5
- token_decay_boost: float32 [4096, 2048], P('sp', 'tp'), may hold values from -0.7 to 0
- output_projection_weight: bfloat16 [2048, 2048], P('tp'), may hold values from -0.375 to 0.375
- expert_norm_gain: float32 [2048], replicated, may hold values from 0.1 to 1.9
- routes: int32 [4096, 2], P('sp'), may hold values from 0 to 7, all different within a row; in each aligned block of 128 rows (0 to 127, 128 to 255, ...) at most 48 rows name the same one
- expert_pair_weight: float32 [4096, 2], P(('sp', 'tp')), may hold values from 0.2 to 0.8
- gate_weight: bfloat16 [8, 2048, 2048], P('sp', None, 'tp'), may hold values from -0.125 to 0.125
- up_weight: bfloat16 [8, 2048, 2048], P('sp', None, 'tp'), may hold values from -0.125 to 0.125
- down_weight: bfloat16 [8, 2048, 2048], P('sp', None, 'tp'), may hold values from -0.25 to 0.25
Outputs:
- layer_out: bfloat16 [4096, 2048], P(('sp', 'tp'))
The draws below stay inside these ranges and needn't reach their ends.
Inputs may be any that keep to these rules, and one draw needn't show every extreme that they name: `routes`: in each aligned block of 128 rows no expert is named by more than 48 rows, and the two experts of a row differ.
All inputs are finite; a program needn't handle non-finite values.
Results may differ from the reference program's by a relative error of at most 0.013.
Values may be sent and summed in bfloat16 or wider, within the bound.
A program may use at most 128 MiB of HBM per device.

```python
import math
import jax
import jax.numpy as jnp
import numpy as np
from jax import lax

D = 2048
LRU = 2048
BW = 64
HID = 2048
CONV = 4
TOK_SP = 512
BLOCKS = 32
TOKENS = 4096
ROWS_DEV = 128
EXPERTS = 8
CAP = 48
ROWS_ALL = 1536


def draw_recurrent_input(key, part):
    base_key, scale_key = jax.random.split(jax.random.fold_in(key, 11))
    base = jnp.clip(jax.random.normal(base_key, (TOKENS, LRU), jnp.float32), -6.0, 6.0)
    block_scale = jnp.exp(jax.random.uniform(scale_key, (TOKENS // TOK_SP, 1), jnp.float32, -0.7, 0.7))
    return (base * jnp.repeat(block_scale, TOK_SP, axis=0)).astype(jnp.bfloat16)


def draw_channel_decay_raw(key, part):
    pick_key, fast_key, slow_key = jax.random.split(jax.random.fold_in(key, 12), 3)
    share = 0.5
    fast = jax.random.uniform(pick_key, (LRU,), jnp.float32) < share
    quick = jax.random.uniform(fast_key, (LRU,), jnp.float32, 4.8, 6.0)
    steady = jax.random.uniform(slow_key, (LRU,), jnp.float32, 11.0, 13.5)
    return jnp.where(fast, quick, steady)


def draw_token_decay_boost(key, part):
    place_key, size_key = jax.random.split(jax.random.fold_in(key, 13))
    places = jax.random.randint(place_key, (3, LRU), 0, TOKENS)
    drops = jax.random.uniform(size_key, (3, LRU), jnp.float32, -0.7, -0.22)
    position = jnp.arange(TOKENS)[:, None]
    result = jnp.zeros((TOKENS, LRU), jnp.float32)
    for number in range(3):
        result = jnp.minimum(result, jnp.where(position == places[number][None, :], drops[number][None, :], 0.0))
    return result


def level_of(key, shape, cuts, least, high):
    loudness, own = 1.0, jax.random.fold_in(key, 6)
    for dim, blocks in cuts:
        steps = jnp.exp(jax.random.uniform(jax.random.fold_in(own, dim), (blocks,), jnp.float32, least / len(cuts), high / len(cuts)))
        loudness = loudness * jnp.repeat(steps, shape[dim] // blocks).reshape([-1 if axis == dim else 1 for axis in range(len(shape))])
    return loudness


def routed_block(own_key, own, number, rows, amount, top, limit, slope):
    ranking = jax.random.permutation(own_key, amount)
    packed, ordinary = shares(amount, rows * top, limit, slope, True), shares(amount, rows * top, limit, slope, False)
    places = jnp.arange(amount)

    def named(tallies, rotation):
        used = int((tallies > 0).sum())
        fixed = max(1, used // 4)
        shifted = fixed + (places - fixed + rotation * (used - fixed)) % max(1, amount - fixed)
        return jnp.zeros((amount,), jnp.int32).at[ranking[jnp.where(places < fixed, places, shifted)]].set(jnp.asarray(tallies, jnp.int32))

    tallies = jnp.where(number % 4 == 0, named(packed, number // 4), named(ordinary, number - number // 4 - 1))
    mixed = jax.random.permutation(jax.random.fold_in(own, 3), amount)
    donor, sink = mixed[0:amount // 2 * 2:2], mixed[1:amount // 2 * 2:2]
    margin = jnp.minimum(tallies[donor] - 1, limit - tallies[sink]) // 2
    margin = jnp.where((donor == ranking[0]) | (sink == ranking[0]) | (tallies[sink] == 0), 0, jnp.maximum(margin, 0))
    shifted = jax.random.randint(jax.random.fold_in(own, 4), (amount // 2,), 0, 1 << 20) % (margin + 1)
    tallies = tallies.at[donor].add(-shifted).at[sink].add(shifted)
    labels = jnp.searchsorted(jnp.cumsum(tallies), jnp.arange(rows * top), side="right").astype(jnp.int32)
    listing = labels.reshape(top, rows).T
    listing = listing[jax.random.permutation(jax.random.fold_in(own, 1), rows)]
    rotation = jax.random.randint(jax.random.fold_in(own, 2), (rows, 1), 0, top)
    return jnp.take_along_axis(listing, (jnp.arange(top)[None, :] + rotation) % top, axis=1)


def shares(amount, total, bound, slope, full):
    portions = [(1 << 20) // math.isqrt(standing ** slope) + 1 for standing in range(1, amount + 1)]
    largest = bound if full else min(bound, max(-(-total // amount), total * portions[0] // sum(portions)))
    least = 1 if total - largest >= amount - 1 else 0
    counts, rest = [largest] + [least] * (amount - 1), total - largest - least * (amount - 1)
    while rest > 0:
        candidates = [i for i in range(1, amount) if counts[i] < largest] or [i for i in range(1, amount) if counts[i] < bound]
        mass, remaining = sum([portions[i] for i in candidates]), rest
        for i in candidates:
            extra = min(bound - counts[i], max(1, remaining * portions[i] // mass), rest)
            counts[i] = counts[i] + extra
            rest = rest - extra
    return np.array(counts)


def normal_values(rng, extent, scale, reach, shards=(), kind=jnp.bfloat16):
    drawn = scale * jax.random.normal(rng, extent, jnp.float32)
    if shards:
        drawn = drawn * level_of(rng, extent, shards, -0.22, 0.18)
    return jnp.clip(drawn, -reach, reach).astype(kind)


def setup_inputs(seed: int = 0) -> dict:
    splits = jax.random.split(jax.random.key(seed), 16)
    resid = normal_values(splits[0], (TOKENS, D), 1.0, 6.0, ((0, 32),))
    recurrent_input = draw_recurrent_input(jax.random.fold_in(splits[15], 71), 0)
    recurrent_out_gate = normal_values(splits[2], (TOKENS, LRU), 1.0, 6.0, ((0, 8), (1, 4)))
    filter_weight = normal_values(splits[3], (CONV, LRU), 0.5, 3.0, ((1, 4),), jnp.float32)
    recurrence_gate_matrix = normal_values(splits[4], (BLOCKS, BW, BW), BW ** -0.5, 0.75, ((0, 4),))
    input_gate_matrix = normal_values(splits[5], (BLOCKS, BW, BW), BW ** -0.5, 0.75, ((0, 4),))
    channel_decay_raw = draw_channel_decay_raw(jax.random.fold_in(splits[15], 71), 0)
    token_decay_boost = draw_token_decay_boost(jax.random.fold_in(splits[15], 71), 0)
    output_projection_weight = normal_values(splits[8], (LRU, D), (LRU // 9) ** -0.5, 0.375, ((0, 4),))
    expert_norm_gain = jnp.clip(1.0 + 0.18 * jax.random.normal(splits[9], (D,), jnp.float32), 0.1, 1.9)
    routes_keys = jax.random.split(jax.random.fold_in(splits[10], 1), TOKENS // ROWS_DEV)
    routes_turns = jax.random.permutation(jax.random.fold_in(splits[10], 3), TOKENS // ROWS_DEV)
    routes = jax.vmap(lambda own, number: routed_block(jax.random.fold_in(splits[10], 2), own, number, ROWS_DEV, EXPERTS, 2, CAP, 1))(routes_keys, routes_turns).reshape((TOKENS, 2))
    expert_pair_weight = jnp.clip(0.2 + 0.6 * jax.random.uniform(splits[11], (TOKENS, 2), jnp.float32) ** level_of(splits[11], (TOKENS, 2), ((0, 32),), -0.2, 0.2), 0.2, 0.8)
    gate_weight = normal_values(splits[12], (EXPERTS, D, HID), D ** -0.5, 0.125, ((0, 8), (2, 4)))
    up_weight = normal_values(splits[13], (EXPERTS, D, HID), D ** -0.5, 0.125, ((0, 8), (2, 4)))
    down_weight = normal_values(splits[14], (EXPERTS, HID, D), (HID // 4) ** -0.5, 0.25, ((0, 8), (2, 4)))
    return dict(resid=resid, recurrent_input=recurrent_input, recurrent_out_gate=recurrent_out_gate, filter_weight=filter_weight, recurrence_gate_matrix=recurrence_gate_matrix, input_gate_matrix=input_gate_matrix, channel_decay_raw=channel_decay_raw, token_decay_boost=token_decay_boost, output_projection_weight=output_projection_weight, expert_norm_gain=expert_norm_gain, routes=routes, expert_pair_weight=expert_pair_weight, gate_weight=gate_weight, up_weight=up_weight, down_weight=down_weight)


def chain_step(earlier, later):
    return (earlier[0] * later[0], later[0] * earlier[1] + later[1])

def reference(resid, recurrent_input, recurrent_out_gate, filter_weight, recurrence_gate_matrix, input_gate_matrix, channel_decay_raw, token_decay_boost, output_projection_weight, expert_norm_gain, routes, expert_pair_weight, gate_weight, up_weight, down_weight):
    total = recurrent_input.shape[0]
    taps = filter_weight.shape[0]
    padded = jnp.pad(recurrent_input.astype(jnp.float32), ((taps - 1, 0), (0, 0)))
    mixed_in = padded[0:total] * filter_weight[0]
    for offset in range(1, taps):
        mixed_in = mixed_in + padded[offset:offset + total] * filter_weight[offset]
    smoothed = mixed_in.astype(jnp.bfloat16)
    grouped = smoothed.astype(jnp.float32).reshape(total, BLOCKS, BW)
    recurrence_gate = jax.nn.sigmoid(jnp.einsum('tni,nij->tnj', grouped, recurrence_gate_matrix.astype(jnp.float32)).reshape(total, LRU))
    input_gate = jax.nn.sigmoid(jnp.einsum('tni,nij->tnj', grouped, input_gate_matrix.astype(jnp.float32)).reshape(total, LRU))
    decay_logarithm = -8.0 * recurrence_gate * jax.nn.softplus(-channel_decay_raw) + token_decay_boost
    decay = jnp.exp(decay_logarithm)
    drive = jnp.sqrt(-jnp.expm1(2.0 * decay_logarithm)) * (input_gate * smoothed.astype(jnp.float32))
    running, state = lax.associative_scan(chain_step, (decay, drive), axis=0)
    branch = (jax.nn.gelu(recurrent_out_gate.astype(jnp.float32)) * state).astype(jnp.bfloat16)
    projected = jnp.dot(branch, output_projection_weight, preferred_element_type=jnp.float32)
    stream = (resid.astype(jnp.float32) + projected).astype(jnp.bfloat16)
    stream_wide = stream.astype(jnp.float32)
    normed = (stream_wide * lax.rsqrt(lax.optimization_barrier(jnp.mean(stream_wide * stream_wide, axis=1, keepdims=True)) + 1e-06) * expert_norm_gain).astype(jnp.bfloat16)
    flat_routes = routes.reshape(-1)
    flat_weight = expert_pair_weight.reshape(-1)
    slot_index = jnp.arange(ROWS_ALL, dtype=jnp.int32)

    def one_expert(accum, items):
        gate_part, up_part, down_part, number = items
        hits = flat_routes == number
        count = jnp.sum(hits.astype(jnp.int32))
        chosen = jnp.nonzero(hits, size=ROWS_ALL, fill_value=0)[0].astype(jnp.int32)
        valid = slot_index < count
        token = chosen // 2
        rows = normed[token]
        gate = jnp.dot(rows, gate_part, preferred_element_type=jnp.float32)
        upward = jnp.dot(rows, up_part, preferred_element_type=jnp.float32)
        active = (jax.nn.silu(gate) * upward).astype(jnp.bfloat16)
        result = jnp.dot(active, down_part, preferred_element_type=jnp.float32).astype(jnp.bfloat16).astype(jnp.float32)
        factor = jnp.where(valid, flat_weight[chosen], 0.0)
        return (accum.at[token].add(result * factor[:, None]), None)
    start = jnp.zeros((total, D), jnp.float32)
    accum, _ = lax.scan(one_expert, start, (gate_weight, up_weight, down_weight, jnp.arange(EXPERTS, dtype=jnp.int32)))
    return (stream_wide + accum).astype(jnp.bfloat16)
```

```python
import contextlib
import functools

import jax
import jax.numpy as jnp
from jax import lax
from jax.experimental import pallas as pl
from jax.experimental.pallas import tpu as pltpu
from jax.sharding import PartitionSpec as P

RECURRENT_SCALE = 8.0
EPSILON = 1e-06
LANES = 128
TILE = 8
CHUNK = 64
RIM = 16
MESH = pl.DeviceIdType.MESH


def at_device(sp, tp):
    return {"device_id": (sp, tp), "device_id_type": MESH}


def one_minus_exp(y):
    series = 1.0 + y * (1 / 2 + y * (1 / 6 + y * (1 / 24 + y * (1 / 120 + y * (1 / 720 + y / 5040)))))
    series = series * -y
    return jnp.where(y > -0.4, series, 1.0 - jnp.exp(y))


def recurrence_kernel(
    sp_size,
    tp_size,
    x_hbm,
    out_gate_hbm,
    taps_hbm,
    recur_map_hbm,
    input_map_hbm,
    decay_hbm,
    boost_hbm,
    weight_hbm,
    resid_hbm,
    gain_hbm,
    stream_ref,
    normed_ref,
    x_ref,
    out_gate_ref,
    taps_ref,
    recur_map_ref,
    input_map_ref,
    decay_ref,
    boost_ref,
    weight_ref,
    resid_ref,
    gain_ref,
    gates_ref,
    ext,
    rim,
    running,
    local,
    lifted,
    totals,
    send_pair,
    recv_pair,
    send_far,
    recv_far,
    summed,
    load_sems,
    rim_sems,
    total_send_sems,
    total_recv_sems,
    pair_send_sems,
    pair_recv_sems,
    far_send_sems,
    far_recv_sems,
):
    sp, tp = lax.axis_index("sp"), lax.axis_index("tp")
    tokens, channels = x_ref.shape
    taps = taps_ref.shape[0]
    width = weight_ref.shape[1]
    rows_dev = resid_ref.shape[0]
    far_size = tp_size // 2
    core, far = lax.rem(tp, 2), tp // 2
    partner = far * 2 + 1 - core

    sources = (
        (x_hbm, x_ref),
        (out_gate_hbm, out_gate_ref),
        (taps_hbm, taps_ref),
        (recur_map_hbm, recur_map_ref),
        (input_map_hbm, input_map_ref),
        (decay_hbm, decay_ref),
        (boost_hbm, boost_ref),
        (weight_hbm, weight_ref),
        (resid_hbm, resid_ref),
        (gain_hbm, gain_ref),
    )
    loads = [
        pltpu.make_async_copy(source, target, load_sems.at[n])
        for n, (source, target) in enumerate(sources)
    ]
    for load in loads:
        load.start()

    barrier = pltpu.get_barrier_semaphore()
    for d in range(1, sp_size):
        pl.semaphore_signal(barrier, inc=1, **at_device(lax.rem(sp + d, sp_size), tp))
    pl.semaphore_signal(barrier, inc=1, **at_device(sp, partner))
    for d in range(1, far_size):
        pl.semaphore_signal(
            barrier, inc=1, **at_device(sp, lax.rem(far + d, far_size) * 2 + core)
        )
    pl.semaphore_wait(barrier, sp_size - 1 + far_size)

    loads[0].wait()
    rim_copy = pltpu.make_async_remote_copy(
        src_ref=x_ref.at[pl.ds(tokens - RIM, RIM)],
        dst_ref=rim,
        send_sem=rim_sems.at[0],
        recv_sem=rim_sems.at[1],
        **at_device(lax.rem(sp + 1, sp_size), tp),
    )
    rim_copy.start()
    loads[1].wait()

    @pl.loop(0, tokens // CHUNK)
    def _(i):
        r = pl.multiple_of(i * CHUNK, CHUNK)
        ext[pl.ds(r + TILE, CHUNK), :] = x_ref[pl.ds(r, CHUNK), :].astype(jnp.float32)
        lifted[pl.ds(r, CHUNK), :] = jax.nn.gelu(out_gate_ref[pl.ds(r, CHUNK), :].astype(jnp.float32))

    for load in loads[2:6]:
        load.wait()
    map_size = recur_map_ref.shape[1]
    per = LANES // map_size
    gates_ref[...] = jnp.zeros_like(gates_ref)
    for b in range(channels // LANES):
        for n in range(per):
            rows = slice(n * map_size, (n + 1) * map_size)
            for side, maps in enumerate((recur_map_ref, input_map_ref)):
                start = side * LANES + n * map_size
                gates_ref[b, rows, start : start + map_size] = maps[b * per + n]
    raw = decay_ref[...]
    small = jnp.exp(-jnp.abs(raw))
    series = small * (1 - small * (1 / 2 - small * (1 / 3 - small * (1 / 4 - small * (1 / 5 - small / 6)))))
    plus = jnp.maximum(-raw, 0.0) + jnp.where(small < 0.05, series, jnp.log(1.0 + small))
    scale = -RECURRENT_SCALE * plus

    rim_copy.wait()
    loads[6].wait()
    edge = rim[...].astype(jnp.float32)[RIM - TILE :, :]
    ext[0:TILE, :] = jnp.where(sp == 0, 0.0, edge)

    tile_row = lax.broadcasted_iota(jnp.int32, (CHUNK, LANES), 0) % TILE

    def chunk(i, carry):
        r = pl.multiple_of(i * CHUNK, CHUNK)
        out = []
        for b in range(channels // LANES):
            cols = slice(b * LANES, (b + 1) * LANES)
            win = ext[pl.ds(r, CHUNK + TILE), cols]
            base = TILE - taps + 1
            mixed = win[base : base + CHUNK] * taps_ref[0:1, cols]
            for k in range(1, taps):
                mixed = mixed + win[base + k : base + k + CHUNK] * taps_ref[k : k + 1, cols]
            smoothed = mixed.astype(jnp.bfloat16)
            both = jnp.dot(smoothed, gates_ref[b], preferred_element_type=jnp.float32)
            recur = jax.nn.sigmoid(both[:, :LANES])
            inward = jax.nn.sigmoid(both[:, LANES:])
            log_decay = recur * scale[0:1, cols] + boost_ref[pl.ds(r, CHUNK), cols]
            a = jnp.exp(log_decay)
            h = jnp.sqrt(one_minus_exp(2.0 * log_decay)) * (inward * smoothed.astype(jnp.float32))
            for s in (1, 2, 4):
                inside = tile_row >= s
                a_before = jnp.where(inside, pltpu.roll(a, s, 0), 1.0)
                h_before = jnp.where(inside, pltpu.roll(h, s, 0), 0.0)
                h = a * h_before + h
                a = a * a_before
            carry_a, carry_h = carry[2 * b], carry[2 * b + 1]
            for t in range(CHUNK // TILE):
                rows = slice(t * TILE, (t + 1) * TILE)
                h_t = h[rows] + a[rows] * carry_h
                a_t = a[rows] * carry_a
                running[pl.ds(r + t * TILE, TILE), cols] = a_t
                local[pl.ds(r + t * TILE, TILE), cols] = h_t
                carry_a, carry_h = a_t[TILE - 1 : TILE], h_t[TILE - 1 : TILE]
            out += [carry_a, carry_h]
        return tuple(out)

    ones, zeros = jnp.ones((1, LANES), jnp.float32), jnp.zeros((1, LANES), jnp.float32)
    last = lax.fori_loop(0, tokens // CHUNK, chunk, (ones, zeros) * (channels // LANES))
    pick = lax.broadcasted_iota(jnp.int32, (TILE, LANES), 0) == 0
    for b in range(channels // LANES):
        totals[sp, :, b * LANES : (b + 1) * LANES] = jnp.where(pick, last[2 * b], last[2 * b + 1])

    sent = []
    for d in range(1, sp_size):
        copy = pltpu.make_async_remote_copy(
            src_ref=totals.at[sp],
            dst_ref=totals.at[sp],
            send_sem=total_send_sems.at[d],
            recv_sem=total_recv_sems.at[d],
            **at_device(lax.rem(sp + d, sp_size), tp),
        )
        copy.start()
        sent.append(copy)
    for copy in sent:
        copy.wait()

    entering = jnp.zeros((1, channels), jnp.float32)
    for k in range(sp_size):
        part = totals[k]
        after = part[0:1] * entering + part[1:2]
        entering = jnp.where(k < sp, after, entering)

    def partial_sum(block, n, step):
        rows = pl.ds(pl.multiple_of(block * rows_dev, rows_dev), rows_dev)
        state = local[rows, :] + running[rows, :] * entering
        branch = (lifted[rows, :] * state).astype(jnp.bfloat16)
        cols = slice(n * step, (n + 1) * step)
        return jnp.dot(branch, weight_ref[:, cols], preferred_element_type=jnp.float32)

    step = 512 if width % 512 == 0 else width
    steps = width // step

    for load in loads[7:]:
        load.wait()
    pair_copies = {}
    for d in range(1, far_size + 1):
        other = lax.rem(far + d, far_size)
        for n in range(steps):
            send_pair[d - 1, n] = partial_sum(other * 2 + 1 - core, n, step).astype(jnp.bfloat16)
            pair_copies[d, n] = pltpu.make_async_remote_copy(
                src_ref=send_pair.at[d - 1, n],
                dst_ref=recv_pair.at[d - 1, n],
                send_sem=pair_send_sems.at[d - 1, n],
                recv_sem=pair_recv_sems.at[d - 1, n],
                **at_device(sp, partner),
            )
            pair_copies[d, n].start()
    far_copies = {}
    for d in range(1, far_size):
        other = lax.rem(far + d, far_size)
        for n in range(steps):
            total = partial_sum(other * 2 + core, n, step)
            pair_copies[d, n].wait_recv()
            total = total + recv_pair[d - 1, n].astype(jnp.float32)
            send_far[d - 1, n] = total.astype(jnp.bfloat16)
            far_copies[d, n] = pltpu.make_async_remote_copy(
                src_ref=send_far.at[d - 1, n],
                dst_ref=recv_far.at[d - 1, n],
                send_sem=far_send_sems.at[d - 1, n],
                recv_sem=far_recv_sems.at[d - 1, n],
                **at_device(sp, other * 2 + core),
            )
            far_copies[d, n].start()

    for n in range(steps):
        cols = slice(n * step, (n + 1) * step)
        total = partial_sum(tp, n, step) + resid_ref[:, cols].astype(jnp.float32)
        pair_copies[far_size, n].wait_recv()
        summed[:, cols] = total + recv_pair[far_size - 1, n].astype(jnp.float32)

    squares = jnp.zeros((rows_dev, 1), jnp.float32)
    for n in range(steps):
        cols = slice(n * step, (n + 1) * step)
        total = summed[:, cols]
        for d in range(1, far_size):
            far_copies[d, n].wait_recv()
            total = total + recv_far[d - 1, n].astype(jnp.float32)
        stream = total.astype(jnp.bfloat16)
        stream_ref[:, cols] = stream
        wide = stream.astype(jnp.float32)
        squares = squares + jnp.sum(wide * wide, axis=1, keepdims=True)
    norm = lax.rsqrt(squares * (1.0 / width) + EPSILON)
    for n in range(steps):
        cols = slice(n * step, (n + 1) * step)
        wide = stream_ref[:, cols].astype(jnp.float32)
        normed_ref[:, cols] = (wide * norm * gain_ref[0:1, cols]).astype(jnp.bfloat16)
    for copy in [*pair_copies.values(), *far_copies.values()]:
        copy.wait_send()


def recurrence(
    resid,
    recurrent_input,
    recurrent_out_gate,
    filter_weight,
    recurrence_gate_matrix,
    input_gate_matrix,
    channel_decay_raw,
    token_decay_boost,
    output_projection_weight,
    expert_norm_gain,
):
    sp_size, tp_size = lax.axis_size("sp"), lax.axis_size("tp")
    tokens, channels = recurrent_input.shape
    rows_dev, width = resid.shape
    far_size = tp_size // 2
    step = 512 if width % 512 == 0 else width
    steps = width // step
    vmem = pl.BlockSpec(memory_space=pltpu.VMEM)
    row_shape = jax.ShapeDtypeStruct((rows_dev, width), jnp.bfloat16)
    wide = pltpu.VMEM((tokens, channels), jnp.float32)
    far_slots = max(1, far_size - 1)
    operands = (
        recurrent_input,
        recurrent_out_gate,
        filter_weight,
        recurrence_gate_matrix,
        input_gate_matrix,
        channel_decay_raw.reshape(1, channels),
        token_decay_boost,
        output_projection_weight,
        resid,
        expert_norm_gain.reshape(1, width),
    )
    return pl.pallas_call(
        functools.partial(recurrence_kernel, sp_size, tp_size),
        out_shape=(row_shape, row_shape),
        in_specs=[pl.BlockSpec(memory_space=pltpu.HBM)] * len(operands),
        out_specs=(vmem, vmem),
        scratch_shapes=[
            *[pltpu.VMEM(operand.shape, operand.dtype) for operand in operands],
            pltpu.VMEM((channels // LANES, LANES, 2 * LANES), jnp.bfloat16),
            pltpu.VMEM((tokens + TILE, channels), jnp.float32),
            pltpu.VMEM((RIM, channels), jnp.bfloat16),
            wide,
            wide,
            wide,
            pltpu.VMEM((sp_size, TILE, channels), jnp.float32),
            pltpu.VMEM((far_size, steps, rows_dev, step), jnp.bfloat16),
            pltpu.VMEM((far_size, steps, rows_dev, step), jnp.bfloat16),
            pltpu.VMEM((far_slots, steps, rows_dev, step), jnp.bfloat16),
            pltpu.VMEM((far_slots, steps, rows_dev, step), jnp.bfloat16),
            pltpu.VMEM((rows_dev, width), jnp.float32),
            pltpu.SemaphoreType.DMA((len(operands),)),
            pltpu.SemaphoreType.DMA((2,)),
            pltpu.SemaphoreType.DMA((sp_size,)),
            pltpu.SemaphoreType.DMA((sp_size,)),
            pltpu.SemaphoreType.DMA((far_size, steps)),
            pltpu.SemaphoreType.DMA((far_size, steps)),
            pltpu.SemaphoreType.DMA((far_slots, steps)),
            pltpu.SemaphoreType.DMA((far_slots, steps)),
        ],
        compiler_params=pltpu.CompilerParams(
            collective_id=0, has_side_effects=True, vmem_limit_bytes=67043328
        ),
    )(*operands)


def slot_numbers(picks, experts):
    flat = picks.reshape(-1)
    onehot = (flat[:, None] == jnp.arange(experts, dtype=jnp.int32)[None, :]).astype(jnp.int32)
    before = jnp.cumsum(onehot, axis=0) - onehot
    return (flat, jnp.sum(before * onehot, axis=1))


def fill_slots(source_rows, slot_of, row_of, slot_count):
    match = slot_of[None, :] == jnp.arange(slot_count, dtype=jnp.int32)[:, None]
    picked = jnp.sum(jnp.where(match, row_of[None, :], 0), axis=1)
    present = jnp.any(match, axis=1)
    return jnp.where(present[:, None], source_rows[picked], jnp.zeros((), source_rows.dtype))


def expert_hidden(rows, gate_weight, up_weight):
    gate = jnp.dot(rows, gate_weight[0], preferred_element_type=jnp.float32)
    upward = jnp.dot(rows, up_weight[0], preferred_element_type=jnp.float32)
    return (jax.nn.silu(gate) * upward).astype(jnp.bfloat16)


def expert_down(active, down_weight):
    columns = down_weight[0]
    return jnp.dot(
        lax.all_gather(active, "tp", axis=1, tiled=True),
        columns,
        preferred_element_type=jnp.float32,
    ).astype(jnp.bfloat16)


def phase(name):
    return contextlib.nullcontext()


def layer_kernel(
    sp_size,
    tp_size,
    capacity,
    x_hbm,
    out_gate_hbm,
    taps_hbm,
    recur_map_hbm,
    input_map_hbm,
    decay_hbm,
    boost_hbm,
    routes_hbm,
    pair_weight_hbm,
    weight_hbm,
    resid_hbm,
    gain_hbm,
    gate_hbm,
    up_hbm,
    down_hbm,
    out_ref,
    x_ref,
    out_gate_ref,
    taps_ref,
    recur_map_ref,
    input_map_ref,
    decay_ref,
    boost_ref,
    routes_ref,
    pair_weight_ref,
    weight_ref,
    resid_ref,
    gain_ref,
    gate,
    up,
    down,
    gates_ref,
    ext,
    rim,
    running,
    local,
    lifted,
    branch,
    totals,
    across,
    along,
    send_pair,
    recv_pair,
    send_far,
    recv_far,
    summed,
    stream_ref,
    normed_ref,
    other_normed,
    own_weights,
    pair_weights,
    ranks,
    choose,
    choose_other,
    mixers,
    outgoing,
    outgoing_other,
    rows,
    active,
    result,
    returned,
    blend,
    gathered,
    load_sems,
    rim_sems,
    total_send,
    total_recv,
    pair_send,
    pair_recv,
    far_send,
    far_recv,
    cross_send,
    cross_recv,
    weight_send,
    weight_recv,
    out_send,
    out_recv,
    near_send,
    near_recv,
    row_far_send,
    row_far_recv,
    row_pair_send,
    row_pair_recv,
    act_far_send,
    act_far_recv,
    act_pair_send,
    act_pair_recv,
    back_send,
    back_recv,
    blend_send,
    blend_recv,
):
    sp, tp = lax.axis_index("sp"), lax.axis_index("tp")
    tokens, channels = x_ref.shape
    taps = taps_ref.shape[0]
    rows_dev, width = resid_ref.shape
    picks = routes_ref.shape[1]
    hidden, columns = gate.shape[1], down.shape[1]
    core, far = lax.rem(tp, 2), tp // 2
    other = 1 - far
    partner = far * 2 + 1 - core
    across_tp = other * 2 + core
    half = sp_size // 2
    steps, step = send_pair.shape[1], send_pair.shape[3]
    pieces = far_send.shape[0]
    piece = rows_dev // pieces

    def flipped(d):
        total, bit = 0, 1
        while bit < sp_size:
            total = total + bit * lax.rem(sp // bit + d // bit, 2)
            bit *= 2
        return total

    sources = (
        (x_hbm, x_ref),
        (out_gate_hbm, out_gate_ref),
        (taps_hbm, taps_ref),
        (recur_map_hbm, recur_map_ref),
        (input_map_hbm, input_map_ref),
        (decay_hbm, decay_ref),
        (boost_hbm, boost_ref),
        (routes_hbm, routes_ref),
        (pair_weight_hbm, pair_weight_ref),
        (weight_hbm, weight_ref),
        (resid_hbm, resid_ref),
        (gain_hbm, gain_ref),
        (gate_hbm.at[0], gate),
        (up_hbm.at[0], up),
        (down_hbm.at[0], down),
    )
    loads = [
        pltpu.make_async_copy(source, target, load_sems.at[n])
        for n, (source, target) in enumerate(sources)
    ]
    for load in loads[:12]:
        load.start()

    barrier = pltpu.get_barrier_semaphore()
    for d in range(1, sp_size):
        pl.semaphore_signal(barrier, inc=1, **at_device(lax.rem(sp + d, sp_size), tp))
    for u in range(1, tp_size):
        pl.semaphore_signal(barrier, inc=1, **at_device(sp, lax.rem(tp + u, tp_size)))

    loads[0].wait()
    chunks = tokens // CHUNK

    @pl.loop(0, chunks)
    def _(i):
        r = pl.multiple_of(i * CHUNK, CHUNK)
        ext[pl.ds(r + TILE, CHUNK), :] = x_ref[pl.ds(r, CHUNK), :].astype(jnp.float32)

    for load in loads[2:6]:
        load.wait()
    map_size = recur_map_ref.shape[1]
    per = LANES // map_size
    gates_ref[...] = jnp.zeros_like(gates_ref)
    for b in range(channels // LANES):
        for n in range(per):
            spots = slice(n * map_size, (n + 1) * map_size)
            for side, maps in enumerate((recur_map_ref, input_map_ref)):
                start = side * LANES + n * map_size
                gates_ref[b, spots, start : start + map_size] = maps[b * per + n]
    raw = decay_ref[...]
    small = jnp.exp(-jnp.abs(raw))
    series = small * (1 - small * (1 / 2 - small * (1 / 3 - small * (1 / 4 - small * (1 / 5 - small / 6)))))
    plus = jnp.maximum(-raw, 0.0) + jnp.where(small < 0.05, series, jnp.log(1.0 + small))
    scale = -RECURRENT_SCALE * plus

    loads[8].wait()
    own_weights[...] = jnp.zeros_like(own_weights)
    own_weights[0:picks, :] = pair_weight_ref[...]
    pair_weights[tp] = own_weights[...]

    with phase("barrier"):
        pl.semaphore_wait(barrier, sp_size - 1 + tp_size - 1)
    rim_copy = pltpu.make_async_remote_copy(
        src_ref=x_ref.at[pl.ds(tokens - RIM, RIM)],
        dst_ref=rim,
        send_sem=rim_sems.at[0],
        recv_sem=rim_sems.at[1],
        **at_device(lax.rem(sp + 1, sp_size), tp),
    )
    rim_copy.start()

    def weight_copy(u):
        return pltpu.make_async_remote_copy(
            src_ref=own_weights,
            dst_ref=pair_weights.at[tp],
            send_sem=weight_send.at[u],
            recv_sem=weight_recv.at[u],
            **at_device(sp, lax.rem(tp + u, tp_size)),
        )

    for u in range(1, tp_size):
        weight_copy(u).start()
    loads[6].wait()
    for load in loads[12:]:
        load.start()

    tile_row = lax.broadcasted_iota(jnp.int32, (CHUNK, LANES), 0) % TILE

    def chunk(i, carry):
        r = pl.multiple_of(i * CHUNK, CHUNK)
        out = []
        for b in range(channels // LANES):
            cols = slice(b * LANES, (b + 1) * LANES)
            win = ext[pl.ds(r, CHUNK + TILE), cols]
            base = TILE - taps + 1
            mixed = win[base : base + CHUNK] * taps_ref[0:1, cols]
            for k in range(1, taps):
                mixed = mixed + win[base + k : base + k + CHUNK] * taps_ref[k : k + 1, cols]
            smoothed = mixed.astype(jnp.bfloat16)
            both = jnp.dot(smoothed, gates_ref[b], preferred_element_type=jnp.float32)
            recur = jax.nn.sigmoid(both[:, :LANES])
            inward = jax.nn.sigmoid(both[:, LANES:])
            log_decay = recur * scale[0:1, cols] + boost_ref[pl.ds(r, CHUNK), cols]
            a = jnp.exp(log_decay)
            h = jnp.sqrt(one_minus_exp(2.0 * log_decay)) * (inward * smoothed.astype(jnp.float32))
            for s in (1, 2, 4):
                inside = tile_row >= s
                a_before = jnp.where(inside, pltpu.roll(a, s, 0), 1.0)
                h_before = jnp.where(inside, pltpu.roll(h, s, 0), 0.0)
                h = a * h_before + h
                a = a * a_before
            carry_a, carry_h = carry[2 * b], carry[2 * b + 1]
            for t in range(CHUNK // TILE):
                spots = slice(t * TILE, (t + 1) * TILE)
                h_t = h[spots] + a[spots] * carry_h
                a_t = a[spots] * carry_a
                running[pl.ds(r + t * TILE, TILE), cols] = a_t
                local[pl.ds(r + t * TILE, TILE), cols] = h_t
                carry_a, carry_h = a_t[TILE - 1 : TILE], h_t[TILE - 1 : TILE]
            out += [carry_a, carry_h]
        return tuple(out)

    ones, zeros = jnp.ones((1, LANES), jnp.float32), jnp.zeros((1, LANES), jnp.float32)
    start = (ones, zeros) * (channels // LANES)
    with phase("scan"):
        rest = lax.fori_loop(1, chunks, chunk, start)
    with phase("rim"):
        rim_copy.wait()
    edge = rim[...].astype(jnp.float32)[RIM - TILE :, :]
    ext[0:TILE, :] = jnp.where(sp == 0, 0.0, edge)
    with phase("head"):
        first = lax.fori_loop(0, 1, chunk, start)
    pick = lax.broadcasted_iota(jnp.int32, (TILE, LANES), 0) == 0
    for b in range(channels // LANES):
        first_a, first_h, rest_a, rest_h = first[2 * b], first[2 * b + 1], rest[2 * b], rest[2 * b + 1]
        totals[sp, :, b * LANES : (b + 1) * LANES] = jnp.where(
            pick, first_a * rest_a, rest_a * first_h + rest_h
        )
    head_a = jnp.concatenate(first[0::2], axis=1)
    head_h = jnp.concatenate(first[1::2], axis=1)

    total_copies = []
    for d in range(1, sp_size):
        copy = pltpu.make_async_remote_copy(
            src_ref=totals.at[sp],
            dst_ref=totals.at[sp],
            send_sem=total_send.at[d],
            recv_sem=total_recv.at[d],
            **at_device(lax.rem(sp + d, sp_size), tp),
        )
        copy.start()
        total_copies.append(copy)

    loads[1].wait()

    with phase("gelu"):

        @pl.loop(0, chunks)
        def _(i):
            r = pl.multiple_of(i * CHUNK, CHUNK)
            lifted[pl.ds(r, CHUNK), :] = jax.nn.gelu(
                out_gate_ref[pl.ds(r, CHUNK), :].astype(jnp.float32)
            )

    for load in loads[9:12]:
        load.wait()
    with phase("totals"):
        for copy in total_copies:
            copy.wait()

    entering = jnp.zeros((1, channels), jnp.float32)
    for k in range(sp_size):
        part = totals[k]
        after = part[0:1] * entering + part[1:2]
        entering = jnp.where(k < sp, after, entering)
    entering_rest = head_a * entering + head_h

    both_rows = 2 * rows_dev

    def fill_branch(side):
        for q in range(both_rows // CHUNK):
            r = pl.multiple_of(side * both_rows + q * CHUNK, CHUNK)
            at = pl.ds(r, CHUNK)
            before = entering_rest
            if q == 0:
                before = jnp.where(side == 0, entering, entering_rest)
            state = local[at, :] + running[at, :] * before
            branch[at, :] = (lifted[at, :] * state).astype(jnp.bfloat16)

    def project(side, target):
        fill_branch(side)
        given = branch[pl.ds(pl.multiple_of(side * both_rows, both_rows), both_rows), :]
        for n in range(steps):
            cols = slice(n * step, (n + 1) * step)
            product = jnp.dot(given, weight_ref[:, cols], preferred_element_type=jnp.float32)
            target[0, :, cols] = product[:rows_dev]
            target[1, :, cols] = product[rows_dev:]

    def pair_copy(k, n):
        return pltpu.make_async_remote_copy(
            src_ref=send_pair.at[k, n],
            dst_ref=recv_pair.at[k, n],
            send_sem=pair_send.at[k, n],
            recv_sem=pair_recv.at[k, n],
            **at_device(sp, partner),
        )

    def send_partner(k, held):
        for n in range(steps):
            cols = slice(n * step, (n + 1) * step)
            send_pair[k, n] = held[1 - core, :, cols].astype(jnp.bfloat16)
            pair_copy(k, n).start()

    with phase("project"):
        project(other, across)
        send_partner(0, across)
        project(far, along)
        send_partner(1, along)

    def far_copy(q):
        return pltpu.make_async_remote_copy(
            src_ref=send_far.at[pl.ds(q * piece, piece)],
            dst_ref=recv_far.at[pl.ds(q * piece, piece)],
            send_sem=far_send.at[q],
            recv_sem=far_recv.at[q],
            **at_device(sp, across_tp),
        )

    with phase("far_send"):
        for n in range(steps):
            pair_copy(0, n).wait_recv()
        for q in range(pieces):
            at = slice(q * piece, (q + 1) * piece)
            for n in range(steps):
                cols = slice(n * step, (n + 1) * step)
                sum_far = across[core, at, cols] + recv_pair[0, n, at, :].astype(jnp.float32)
                send_far[at, cols] = sum_far.astype(jnp.bfloat16)
            far_copy(q).start()
    for n in range(steps):
        cols = slice(n * step, (n + 1) * step)
        pair_copy(1, n).wait_recv()
        summed[:, cols] = (
            along[core, :, cols]
            + resid_ref[:, cols].astype(jnp.float32)
            + recv_pair[1, n].astype(jnp.float32)
        )

    slot_row = lax.broadcasted_iota(jnp.int32, (capacity, rows_dev), 0)
    expert_row = lax.broadcasted_iota(jnp.int32, (sp_size, rows_dev), 0)
    earlier = lax.broadcasted_iota(jnp.int32, (rows_dev, rows_dev), 0) < lax.broadcasted_iota(
        jnp.int32, (rows_dev, rows_dev), 1
    )
    earlier = jnp.where(earlier, 1.0, 0.0).astype(jnp.bfloat16)

    loads[7].wait()

    @pl.loop(0, tp_size)
    def _(block):
        chosen = routes_ref[block]
        hits = jnp.zeros((sp_size, rows_dev), jnp.float32)
        for k in range(picks):
            hits = hits + jnp.where(expert_row == chosen[k : k + 1], 1.0, 0.0)
        ranks[block] = jnp.dot(hits.astype(jnp.bfloat16), earlier, preferred_element_type=jnp.float32)

    def selector(block, expert, values):
        chosen = routes_ref[block]
        value = jnp.zeros((1, rows_dev), jnp.float32)
        for k in range(picks):
            value = value + jnp.where(chosen[k : k + 1] == expert, values[k : k + 1], 0.0)
        rank = ranks[block, pl.ds(expert, 1), :].astype(jnp.int32)
        return jnp.where(rank == slot_row, value, 0.0)

    def slot_rows(block):
        return pl.ds(pl.multiple_of(block * capacity, capacity), capacity)

    unit = jnp.ones((picks, rows_dev), jnp.float32)

    @pl.loop(0, sp_size)
    def _(d):
        choose[slot_rows(d), :] = selector(tp, flipped(d), unit).astype(jnp.bfloat16)

    @pl.loop(0, half)
    def _(d):
        choose_other[slot_rows(d), :] = selector(across_tp, flipped(d), unit).astype(jnp.bfloat16)

    with phase("weights"):
        for u in range(1, tp_size):
            weight_copy(u).wait_recv()

    with phase("mixers"):

        @pl.loop(0, tp_size)
        def _(block):
            weight = pair_weights[block]
            coarse = weight.astype(jnp.bfloat16).astype(jnp.float32)
            for n, values in enumerate((coarse, weight - coarse)):
                picked = [selector(block, e, values) for e in range(sp_size)]
                mixers[block, n] = jnp.concatenate(picked, axis=0).T.astype(jnp.bfloat16)

    def cross_copy(q):
        return pltpu.make_async_remote_copy(
            src_ref=normed_ref.at[pl.ds(q * piece, piece)],
            dst_ref=other_normed.at[pl.ds(q * piece, piece)],
            send_sem=cross_send.at[q],
            recv_sem=cross_recv.at[q],
            **at_device(sp, across_tp),
        )

    with phase("norm"):
        for q in range(pieces):
            at = slice(q * piece, (q + 1) * piece)
            far_copy(q).wait_recv()
            squares = jnp.zeros((piece, 1), jnp.float32)
            for n in range(steps):
                cols = slice(n * step, (n + 1) * step)
                stream = (summed[at, cols] + recv_far[at, cols].astype(jnp.float32)).astype(jnp.bfloat16)
                stream_ref[at, cols] = stream
                wide = stream.astype(jnp.float32)
                squares = squares + jnp.sum(wide * wide, axis=1, keepdims=True)
            norm = lax.rsqrt(squares * (1.0 / width) + EPSILON)
            for n in range(steps):
                cols = slice(n * step, (n + 1) * step)
                wide = stream_ref[at, cols].astype(jnp.float32)
                normed_ref[at, cols] = (wide * norm * gain_ref[0:1, cols]).astype(jnp.bfloat16)
            cross_copy(q).start()

    def out_copy(d):
        return pltpu.make_async_remote_copy(
            src_ref=outgoing.at[slot_rows(d)],
            dst_ref=rows.at[sp, slot_rows(tp)],
            send_sem=out_send.at[d],
            recv_sem=out_recv.at[d],
            **at_device(flipped(d), tp),
        )

    def near_copy(d):
        return pltpu.make_async_remote_copy(
            src_ref=outgoing_other.at[slot_rows(d)],
            dst_ref=rows.at[sp, slot_rows(across_tp)],
            send_sem=near_send.at[d],
            recv_sem=near_recv.at[d],
            **at_device(flipped(d), tp),
        )

    def row_far(d):
        place = rows.at[flipped(d), slot_rows(tp)]
        return pltpu.make_async_remote_copy(
            src_ref=place,
            dst_ref=place,
            send_sem=row_far_send.at[d],
            recv_sem=row_far_recv.at[d],
            **at_device(sp, across_tp),
        )

    def row_pair(d, j):
        place = rows.at[flipped(d), slot_rows(across_tp if j else tp)]
        return pltpu.make_async_remote_copy(
            src_ref=place,
            dst_ref=place,
            send_sem=row_pair_send.at[d, j],
            recv_sem=row_pair_recv.at[d, j],
            **at_device(sp, partner),
        )

    def act_far(d):
        place = active.at[flipped(d), tp]
        return pltpu.make_async_remote_copy(
            src_ref=place,
            dst_ref=place,
            send_sem=act_far_send.at[d],
            recv_sem=act_far_recv.at[d],
            **at_device(sp, across_tp),
        )

    def act_pair(d, j):
        place = active.at[flipped(d), across_tp if j else tp]
        return pltpu.make_async_remote_copy(
            src_ref=place,
            dst_ref=place,
            send_sem=act_pair_send.at[d, j],
            recv_sem=act_pair_recv.at[d, j],
            **at_device(sp, partner),
        )

    def back_copy(d):
        return pltpu.make_async_remote_copy(
            src_ref=result.at[d],
            dst_ref=returned.at[sp],
            send_sem=back_send.at[d],
            recv_sem=back_recv.at[d],
            **at_device(flipped(d), tp),
        )

    mates = (across_tp, other * 2 + 1 - core, partner)

    def blend_copy(u):
        return pltpu.make_async_remote_copy(
            src_ref=blend.at[u],
            dst_ref=gathered.at[tp],
            send_sem=blend_send.at[u],
            recv_sem=blend_recv.at[u],
            **at_device(sp, mates[u]),
        )

    pack_rows = half * capacity

    def pack(chooser, given, first_slot, target, first_row):
        picked = chooser[first_slot : first_slot + pack_rows, :]
        for n in range(steps):
            cols = slice(n * step, (n + 1) * step)
            target[first_row : first_row + pack_rows, cols] = jnp.dot(
                picked, given[:, cols], preferred_element_type=jnp.float32
            ).astype(jnp.bfloat16)

    with phase("pack"):
        pack(choose, normed_ref, pack_rows, outgoing, pack_rows)
        for d in range(half, sp_size):
            out_copy(d).start()
        pack(choose, normed_ref, 0, outgoing, 0)
        for d in range(1, half):
            out_copy(d).start()
        rows[sp, slot_rows(tp), :] = outgoing[0:capacity, :]
        row_pair(0, 0).start()
    with phase("cross"):
        for q in range(pieces):
            cross_copy(q).wait_recv()
    with phase("pack_other"):
        pack(choose_other, other_normed, 0, outgoing_other, 0)
        for d in range(1, half):
            near_copy(d).start()
        rows[sp, slot_rows(across_tp), :] = outgoing_other[0:capacity, :]
        row_pair(0, 1).start()

    for load in loads[12:]:
        load.wait()

    def is_near(i):
        return lax.rem(i, 2)

    def group(i):
        near = lax.rem(i, 2)
        return near * lax.rem((i + 1) // 2, half) + (1 - near) * (half + i // 2)

    @pl.loop(0, sp_size + 4)
    def _(s):
        @pl.when((s < sp_size) & (is_near(s) == 0))
        def _():
            d = group(s)
            with phase("w_out"):
                out_copy(d).wait_recv()
            row_far(d).start()
            row_pair(d, 0).start()

        @pl.when((s < sp_size - 1) & (is_near(s) == 1))
        def _():
            d = group(s)
            with phase("w_near"):
                out_copy(d).wait_recv()
                row_pair(d, 0).start()
                near_copy(d).wait_recv()
                row_pair(d, 1).start()

        @pl.when((s >= 2) & (s < sp_size + 2))
        def _():
            d = group(s - 2)
            with phase("w_rowpair"):
                row_pair(d, 0).wait_recv()
                row_pair(d, 1).wait_recv()
            source = flipped(d)
            given = rows[source]
            gated = jnp.dot(given, gate[...], preferred_element_type=jnp.float32)
            upward = jnp.dot(given, up[...], preferred_element_type=jnp.float32)
            active[source, tp] = (jax.nn.silu(gated) * upward).astype(jnp.bfloat16)
            act_far(d).start()
            act_pair(d, 0).start()

        @pl.when((s >= 3) & (s < sp_size + 3))
        def _():
            d = group(s - 3)
            with phase("w_actfar"):
                act_far(d).wait_recv()
            act_pair(d, 1).start()

        @pl.when((s >= 1) & (s < sp_size + 1) & (is_near(s) == 1))
        def _():
            d = group(s - 1)
            with phase("w_rowfar"):
                row_far(d).wait_recv()
            row_pair(d, 1).start()

        @pl.when(s >= 4)
        def _():
            d = group(s - 4)
            with phase("w_actpair"):
                act_pair(d, 0).wait_recv()
                act_pair(d, 1).wait_recv()
            source = flipped(d)
            total = jnp.dot(active[source, 0], down[0:hidden, :], preferred_element_type=jnp.float32)
            for t in range(1, tp_size):
                total = total + jnp.dot(
                    active[source, t],
                    down[t * hidden : (t + 1) * hidden, :],
                    preferred_element_type=jnp.float32,
                )
            result[d] = total.astype(jnp.bfloat16)

            @pl.when(d == 0)
            def _():
                returned[sp] = total.astype(jnp.bfloat16)

            @pl.when(d > 0)
            def _():
                back_copy(d).start()

    with phase("w_back"):

        @pl.loop(1, sp_size)
        def _(d):
            back_copy(d).wait_recv()

    def blended(block):
        part = returned[:, slot_rows(block), :].reshape(sp_size * capacity, columns)
        total = jnp.dot(mixers[block, 0], part, preferred_element_type=jnp.float32)
        total = total + jnp.dot(mixers[block, 1], part, preferred_element_type=jnp.float32)
        return total.astype(jnp.bfloat16)

    with phase("blend"):
        for u, mate in enumerate(mates):
            blend[u] = blended(mate)
            blend_copy(u).start()
        gathered[tp] = blended(tp)
    with phase("w_blend"):
        for u in range(tp_size - 1):
            blend_copy(u).wait_recv()
    for t in range(tp_size):
        cols = slice(t * columns, (t + 1) * columns)
        out_ref[:, cols] = (
            stream_ref[:, cols].astype(jnp.float32) + gathered[t].astype(jnp.float32)
        ).astype(jnp.bfloat16)

    for k in range(2):
        for n in range(steps):
            pair_copy(k, n).wait_send()
    for q in range(pieces):
        far_copy(q).wait_send()
        cross_copy(q).wait_send()
    for u in range(1, tp_size):
        weight_copy(u).wait_send()
    for u in range(tp_size - 1):
        blend_copy(u).wait_send()

    @pl.loop(1, sp_size)
    def _(d):
        out_copy(d).wait_send()
        back_copy(d).wait_send()

    @pl.loop(1, half)
    def _(d):
        near_copy(d).wait_send()

    @pl.loop(half, sp_size)
    def _(d):
        row_far(d).wait_send()

    @pl.loop(0, sp_size)
    def _(d):
        act_far(d).wait_send()
        for j in range(2):
            row_pair(d, j).wait_send()
            act_pair(d, j).wait_send()


def fused_layer(
    resid,
    recurrent_input,
    recurrent_out_gate,
    filter_weight,
    recurrence_gate_matrix,
    input_gate_matrix,
    channel_decay_raw,
    token_decay_boost,
    output_projection_weight,
    expert_norm_gain,
    routes,
    expert_pair_weight,
    gate_weight,
    up_weight,
    down_weight,
    capacity,
):
    sp_size, tp_size = lax.axis_size("sp"), lax.axis_size("tp")
    tokens, channels = recurrent_input.shape
    rows_dev, width = resid.shape
    hidden, columns = gate_weight.shape[2], down_weight.shape[2]
    step = 512 if width % 512 == 0 else width
    steps = width // step
    pieces = 4 if rows_dev % (4 * RIM) == 0 else 1
    half = sp_size // 2
    slots_all = tp_size * capacity
    narrow = (
        recurrent_input,
        recurrent_out_gate,
        filter_weight,
        recurrence_gate_matrix,
        input_gate_matrix,
        channel_decay_raw.reshape(1, channels),
        token_decay_boost,
        routes.reshape(tp_size, rows_dev, -1).swapaxes(1, 2),
        expert_pair_weight.T,
        output_projection_weight,
        resid,
        expert_norm_gain.reshape(1, width),
    )
    operands = (*narrow, gate_weight, up_weight, down_weight)
    dma = pltpu.SemaphoreType.DMA

    def buffer(*shape):
        return pltpu.VMEM(shape, jnp.bfloat16)

    def wide(*shape):
        return pltpu.VMEM(shape, jnp.float32)

    return pl.pallas_call(
        functools.partial(layer_kernel, sp_size, tp_size, capacity),
        out_shape=jax.ShapeDtypeStruct((rows_dev, width), jnp.bfloat16),
        in_specs=[pl.BlockSpec(memory_space=pltpu.HBM)] * len(operands),
        out_specs=pl.BlockSpec(memory_space=pltpu.VMEM),
        scratch_shapes=[
            *[pltpu.VMEM(operand.shape, operand.dtype) for operand in narrow],
            buffer(*gate_weight.shape[1:]),
            buffer(*up_weight.shape[1:]),
            buffer(*down_weight.shape[1:]),
            buffer(channels // LANES, LANES, 2 * LANES),
            wide(tokens + TILE, channels),
            buffer(RIM, channels),
            wide(tokens, channels),
            wide(tokens, channels),
            wide(tokens, channels),
            buffer(tokens, channels),
            wide(sp_size, TILE, channels),
            wide(2, rows_dev, width),
            wide(2, rows_dev, width),
            buffer(2, steps, rows_dev, step),
            buffer(2, steps, rows_dev, step),
            buffer(rows_dev, width),
            buffer(rows_dev, width),
            wide(rows_dev, width),
            buffer(rows_dev, width),
            buffer(rows_dev, width),
            buffer(rows_dev, width),
            wide(TILE, rows_dev),
            wide(tp_size, TILE, rows_dev),
            wide(tp_size, sp_size, rows_dev),
            buffer(sp_size * capacity, rows_dev),
            buffer(half * capacity, rows_dev),
            buffer(tp_size, 2, rows_dev, sp_size * capacity),
            buffer(sp_size * capacity, width),
            buffer(half * capacity, width),
            buffer(sp_size, slots_all, width),
            buffer(sp_size, tp_size, slots_all, hidden),
            buffer(sp_size, slots_all, columns),
            buffer(sp_size, slots_all, columns),
            buffer(tp_size - 1, rows_dev, columns),
            buffer(tp_size, rows_dev, columns),
            dma((len(operands),)),
            dma((2,)),
            dma((sp_size,)),
            dma((sp_size,)),
            dma((2, steps)),
            dma((2, steps)),
            dma((pieces,)),
            dma((pieces,)),
            dma((pieces,)),
            dma((pieces,)),
            dma((tp_size,)),
            dma((tp_size,)),
            dma((sp_size,)),
            dma((sp_size,)),
            dma((half,)),
            dma((half,)),
            dma((sp_size,)),
            dma((sp_size,)),
            dma((sp_size, 2)),
            dma((sp_size, 2)),
            dma((sp_size,)),
            dma((sp_size,)),
            dma((sp_size, 2)),
            dma((sp_size, 2)),
            dma((sp_size,)),
            dma((sp_size,)),
            dma((tp_size - 1,)),
            dma((tp_size - 1,)),
        ],
        compiler_params=pltpu.CompilerParams(
            collective_id=1, has_side_effects=True, vmem_limit_bytes=67043328
        ),
    )(*operands)


def body(
    resid,
    recurrent_input,
    recurrent_out_gate,
    filter_weight,
    recurrence_gate_matrix,
    input_gate_matrix,
    channel_decay_raw,
    token_decay_boost,
    output_projection_weight,
    expert_norm_gain,
    routes,
    expert_pair_weight,
    gate_weight,
    up_weight,
    down_weight,
):
    tp_size = lax.axis_size("tp")
    experts = lax.axis_size("sp")
    rows_dev, model_width = resid.shape
    capacity = max(2, 3 * rows_dev // experts)
    fits = capacity % RIM == 0 and rows_dev % LANES == 0
    if fits and tp_size == 4 and experts >= 4 and experts & (experts - 1) == 0:
        return fused_layer(
            resid,
            recurrent_input,
            recurrent_out_gate,
            filter_weight,
            recurrence_gate_matrix,
            input_gate_matrix,
            channel_decay_raw,
            token_decay_boost,
            output_projection_weight,
            expert_norm_gain,
            routes,
            expert_pair_weight,
            gate_weight,
            up_weight,
            down_weight,
            capacity,
        )
    stream, normed = recurrence(
        resid,
        recurrent_input,
        recurrent_out_gate,
        filter_weight,
        recurrence_gate_matrix,
        input_gate_matrix,
        channel_decay_raw,
        token_decay_boost,
        output_projection_weight,
        expert_norm_gain,
    )
    stream_wide = stream.astype(jnp.float32)
    own_routes = lax.dynamic_slice_in_dim(routes, lax.axis_index("tp") * rows_dev, rows_dev, 0)
    own_flat, own_rank = slot_numbers(own_routes, experts)
    own_slots = own_flat * capacity + own_rank
    row_of = jnp.arange(2 * rows_dev, dtype=jnp.int32) // 2
    outgoing = fill_slots(normed, own_slots, row_of, experts * capacity).reshape(
        experts, capacity, model_width
    )
    arrived = lax.all_to_all(outgoing, "sp", split_axis=0, concat_axis=0, tiled=True)
    piece = lax.all_gather(
        arrived.reshape(1, experts * capacity, model_width), "tp", axis=0, tiled=True
    )
    flat_rows = piece.reshape(piece.shape[0] * piece.shape[1], model_width)
    active = expert_hidden(flat_rows, gate_weight, up_weight).reshape(
        piece.shape[0], piece.shape[1], -1
    )
    result = expert_down(active.reshape(-1, active.shape[2]), down_weight)
    joined = lax.all_to_all(
        result.reshape(tp_size, experts * capacity, -1),
        "tp",
        split_axis=0,
        concat_axis=2,
        tiled=True,
    )
    returned = lax.all_to_all(
        joined.reshape(experts, capacity, model_width),
        "sp",
        split_axis=0,
        concat_axis=0,
        tiled=True,
    )
    picked = (
        returned.reshape(experts * capacity, model_width)[own_slots]
        .astype(jnp.float32)
        .reshape(rows_dev, 2, model_width)
    )
    blended = jnp.sum(picked * expert_pair_weight[:, :, None], axis=1)
    return (stream_wide + blended).astype(jnp.bfloat16)


def solution(mesh):
    placed = (
        P(("sp", "tp"), None),
        P("sp", "tp"),
        P("sp", "tp"),
        P(None, "tp"),
        P("tp", None, None),
        P("tp", None, None),
        P("tp"),
        P("sp", "tp"),
        P("tp", None),
        P(),
        P("sp", None),
        P(("sp", "tp"), None),
        P("sp", None, "tp"),
        P("sp", None, "tp"),
        P("sp", None, "tp"),
    )
    return jax.shard_map(
        body, mesh=mesh, in_specs=placed, out_specs=P(("sp", "tp"), None), check_vma=False
    )
```

```python
import contextlib
import functools

import jax
import jax.numpy as jnp
from jax import lax
from jax.experimental import pallas as pl
from jax.experimental.pallas import tpu as pltpu
from jax.sharding import PartitionSpec as P

RECURRENT_SCALE = 8.0
EPSILON = 1e-06
LANES = 128
TILE = 8
CHUNK = 64
RIM = 16
MESH = pl.DeviceIdType.MESH


def at_device(sp, tp):
    return {"device_id": (sp, tp), "device_id_type": MESH}


def one_minus_exp(y):
    series = 1.0 + y * (1 / 2 + y * (1 / 6 + y * (1 / 24 + y * (1 / 120 + y * (1 / 720 + y / 5040)))))
    series = series * -y
    return jnp.where(y > -0.4, series, 1.0 - jnp.exp(y))


def recurrence_kernel(
    sp_size,
    tp_size,
    x_hbm,
    out_gate_hbm,
    taps_hbm,
    recur_map_hbm,
    input_map_hbm,
    decay_hbm,
    boost_hbm,
    weight_hbm,
    resid_hbm,
    gain_hbm,
    stream_ref,
    normed_ref,
    x_ref,
    out_gate_ref,
    taps_ref,
    recur_map_ref,
    input_map_ref,
    decay_ref,
    boost_ref,
    weight_ref,
    resid_ref,
    gain_ref,
    gates_ref,
    ext,
    rim,
    running,
    local,
    lifted,
    totals,
    send_pair,
    recv_pair,
    send_far,
    recv_far,
    summed,
    load_sems,
    rim_sems,
    total_send_sems,
    total_recv_sems,
    pair_send_sems,
    pair_recv_sems,
    far_send_sems,
    far_recv_sems,
):
    sp, tp = lax.axis_index("sp"), lax.axis_index("tp")
    tokens, channels = x_ref.shape
    taps = taps_ref.shape[0]
    width = weight_ref.shape[1]
    rows_dev = resid_ref.shape[0]
    far_size = tp_size // 2
    core, far = lax.rem(tp, 2), tp // 2
    partner = far * 2 + 1 - core

    sources = (
        (x_hbm, x_ref),
        (out_gate_hbm, out_gate_ref),
        (taps_hbm, taps_ref),
        (recur_map_hbm, recur_map_ref),
        (input_map_hbm, input_map_ref),
        (decay_hbm, decay_ref),
        (boost_hbm, boost_ref),
        (weight_hbm, weight_ref),
        (resid_hbm, resid_ref),
        (gain_hbm, gain_ref),
    )
    loads = [
        pltpu.make_async_copy(source, target, load_sems.at[n])
        for n, (source, target) in enumerate(sources)
    ]
    for load in loads:
        load.start()

    barrier = pltpu.get_barrier_semaphore()
    for d in range(1, sp_size):
        pl.semaphore_signal(barrier, inc=1, **at_device(lax.rem(sp + d, sp_size), tp))
    pl.semaphore_signal(barrier, inc=1, **at_device(sp, partner))
    for d in range(1, far_size):
        pl.semaphore_signal(
            barrier, inc=1, **at_device(sp, lax.rem(far + d, far_size) * 2 + core)
        )
    pl.semaphore_wait(barrier, sp_size - 1 + far_size)

    loads[0].wait()
    rim_copy = pltpu.make_async_remote_copy(
        src_ref=x_ref.at[pl.ds(tokens - RIM, RIM)],
        dst_ref=rim,
        send_sem=rim_sems.at[0],
        recv_sem=rim_sems.at[1],
        **at_device(lax.rem(sp + 1, sp_size), tp),
    )
    rim_copy.start()
    loads[1].wait()

    @pl.loop(0, tokens // CHUNK)
    def _(i):
        r = pl.multiple_of(i * CHUNK, CHUNK)
        ext[pl.ds(r + TILE, CHUNK), :] = x_ref[pl.ds(r, CHUNK), :].astype(jnp.float32)
        lifted[pl.ds(r, CHUNK), :] = jax.nn.gelu(out_gate_ref[pl.ds(r, CHUNK), :].astype(jnp.float32))

    for load in loads[2:6]:
        load.wait()
    map_size = recur_map_ref.shape[1]
    per = LANES // map_size
    gates_ref[...] = jnp.zeros_like(gates_ref)
    for b in range(channels // LANES):
        for n in range(per):
            rows = slice(n * map_size, (n + 1) * map_size)
            for side, maps in enumerate((recur_map_ref, input_map_ref)):
                start = side * LANES + n * map_size
                gates_ref[b, rows, start : start + map_size] = maps[b * per + n]
    raw = decay_ref[...]
    small = jnp.exp(-jnp.abs(raw))
    series = small * (1 - small * (1 / 2 - small * (1 / 3 - small * (1 / 4 - small * (1 / 5 - small / 6)))))
    plus = jnp.maximum(-raw, 0.0) + jnp.where(small < 0.05, series, jnp.log(1.0 + small))
    scale = -RECURRENT_SCALE * plus

    rim_copy.wait()
    loads[6].wait()
    edge = rim[...].astype(jnp.float32)[RIM - TILE :, :]
    ext[0:TILE, :] = jnp.where(sp == 0, 0.0, edge)

    tile_row = lax.broadcasted_iota(jnp.int32, (CHUNK, LANES), 0) % TILE

    def chunk(i, carry):
        r = pl.multiple_of(i * CHUNK, CHUNK)
        out = []
        for b in range(channels // LANES):
            cols = slice(b * LANES, (b + 1) * LANES)
            win = ext[pl.ds(r, CHUNK + TILE), cols]
            base = TILE - taps + 1
            mixed = win[base : base + CHUNK] * taps_ref[0:1, cols]
            for k in range(1, taps):
                mixed = mixed + win[base + k : base + k + CHUNK] * taps_ref[k : k + 1, cols]
            smoothed = mixed.astype(jnp.bfloat16)
            both = jnp.dot(smoothed, gates_ref[b], preferred_element_type=jnp.float32)
            recur = jax.nn.sigmoid(both[:, :LANES])
            inward = jax.nn.sigmoid(both[:, LANES:])
            log_decay = recur * scale[0:1, cols] + boost_ref[pl.ds(r, CHUNK), cols]
            a = jnp.exp(log_decay)
            h = jnp.sqrt(one_minus_exp(2.0 * log_decay)) * (inward * smoothed.astype(jnp.float32))
            for s in (1, 2, 4):
                inside = tile_row >= s
                a_before = jnp.where(inside, pltpu.roll(a, s, 0), 1.0)
                h_before = jnp.where(inside, pltpu.roll(h, s, 0), 0.0)
                h = a * h_before + h
                a = a * a_before
            carry_a, carry_h = carry[2 * b], carry[2 * b + 1]
            for t in range(CHUNK // TILE):
                rows = slice(t * TILE, (t + 1) * TILE)
                h_t = h[rows] + a[rows] * carry_h
                a_t = a[rows] * carry_a
                running[pl.ds(r + t * TILE, TILE), cols] = a_t
                local[pl.ds(r + t * TILE, TILE), cols] = h_t
                carry_a, carry_h = a_t[TILE - 1 : TILE], h_t[TILE - 1 : TILE]
            out += [carry_a, carry_h]
        return tuple(out)

    ones, zeros = jnp.ones((1, LANES), jnp.float32), jnp.zeros((1, LANES), jnp.float32)
    last = lax.fori_loop(0, tokens // CHUNK, chunk, (ones, zeros) * (channels // LANES))
    pick = lax.broadcasted_iota(jnp.int32, (TILE, LANES), 0) == 0
    for b in range(channels // LANES):
        totals[sp, :, b * LANES : (b + 1) * LANES] = jnp.where(pick, last[2 * b], last[2 * b + 1])

    sent = []
    for d in range(1, sp_size):
        copy = pltpu.make_async_remote_copy(
            src_ref=totals.at[sp],
            dst_ref=totals.at[sp],
            send_sem=total_send_sems.at[d],
            recv_sem=total_recv_sems.at[d],
            **at_device(lax.rem(sp + d, sp_size), tp),
        )
        copy.start()
        sent.append(copy)
    for copy in sent:
        copy.wait()

    entering = jnp.zeros((1, channels), jnp.float32)
    for k in range(sp_size):
        part = totals[k]
        after = part[0:1] * entering + part[1:2]
        entering = jnp.where(k < sp, after, entering)

    def partial_sum(block, n, step):
        rows = pl.ds(pl.multiple_of(block * rows_dev, rows_dev), rows_dev)
        state = local[rows, :] + running[rows, :] * entering
        branch = (lifted[rows, :] * state).astype(jnp.bfloat16)
        cols = slice(n * step, (n + 1) * step)
        return jnp.dot(branch, weight_ref[:, cols], preferred_element_type=jnp.float32)

    step = 512 if width % 512 == 0 else width
    steps = width // step

    for load in loads[7:]:
        load.wait()
    pair_copies = {}
    for d in range(1, far_size + 1):
        other = lax.rem(far + d, far_size)
        for n in range(steps):
            send_pair[d - 1, n] = partial_sum(other * 2 + 1 - core, n, step).astype(jnp.bfloat16)
            pair_copies[d, n] = pltpu.make_async_remote_copy(
                src_ref=send_pair.at[d - 1, n],
                dst_ref=recv_pair.at[d - 1, n],
                send_sem=pair_send_sems.at[d - 1, n],
                recv_sem=pair_recv_sems.at[d - 1, n],
                **at_device(sp, partner),
            )
            pair_copies[d, n].start()
    far_copies = {}
    for d in range(1, far_size):
        other = lax.rem(far + d, far_size)
        for n in range(steps):
            total = partial_sum(other * 2 + core, n, step)
            pair_copies[d, n].wait_recv()
            total = total + recv_pair[d - 1, n].astype(jnp.float32)
            send_far[d - 1, n] = total.astype(jnp.bfloat16)
            far_copies[d, n] = pltpu.make_async_remote_copy(
                src_ref=send_far.at[d - 1, n],
                dst_ref=recv_far.at[d - 1, n],
                send_sem=far_send_sems.at[d - 1, n],
                recv_sem=far_recv_sems.at[d - 1, n],
                **at_device(sp, other * 2 + core),
            )
            far_copies[d, n].start()

    for n in range(steps):
        cols = slice(n * step, (n + 1) * step)
        total = partial_sum(tp, n, step) + resid_ref[:, cols].astype(jnp.float32)
        pair_copies[far_size, n].wait_recv()
        summed[:, cols] = total + recv_pair[far_size - 1, n].astype(jnp.float32)

    squares = jnp.zeros((rows_dev, 1), jnp.float32)
    for n in range(steps):
        cols = slice(n * step, (n + 1) * step)
        total = summed[:, cols]
        for d in range(1, far_size):
            far_copies[d, n].wait_recv()
            total = total + recv_far[d - 1, n].astype(jnp.float32)
        stream = total.astype(jnp.bfloat16)
        stream_ref[:, cols] = stream
        wide = stream.astype(jnp.float32)
        squares = squares + jnp.sum(wide * wide, axis=1, keepdims=True)
    norm = lax.rsqrt(squares * (1.0 / width) + EPSILON)
    for n in range(steps):
        cols = slice(n * step, (n + 1) * step)
        wide = stream_ref[:, cols].astype(jnp.float32)
        normed_ref[:, cols] = (wide * norm * gain_ref[0:1, cols]).astype(jnp.bfloat16)
    for copy in [*pair_copies.values(), *far_copies.values()]:
        copy.wait_send()


def recurrence(
    resid,
    recurrent_input,
    recurrent_out_gate,
    filter_weight,
    recurrence_gate_matrix,
    input_gate_matrix,
    channel_decay_raw,
    token_decay_boost,
    output_projection_weight,
    expert_norm_gain,
):
    sp_size, tp_size = lax.axis_size("sp"), lax.axis_size("tp")
    tokens, channels = recurrent_input.shape
    rows_dev, width = resid.shape
    far_size = tp_size // 2
    step = 512 if width % 512 == 0 else width
    steps = width // step
    vmem = pl.BlockSpec(memory_space=pltpu.VMEM)
    row_shape = jax.ShapeDtypeStruct((rows_dev, width), jnp.bfloat16)
    wide = pltpu.VMEM((tokens, channels), jnp.float32)
    far_slots = max(1, far_size - 1)
    operands = (
        recurrent_input,
        recurrent_out_gate,
        filter_weight,
        recurrence_gate_matrix,
        input_gate_matrix,
        channel_decay_raw.reshape(1, channels),
        token_decay_boost,
        output_projection_weight,
        resid,
        expert_norm_gain.reshape(1, width),
    )
    return pl.pallas_call(
        functools.partial(recurrence_kernel, sp_size, tp_size),
        out_shape=(row_shape, row_shape),
        in_specs=[pl.BlockSpec(memory_space=pltpu.HBM)] * len(operands),
        out_specs=(vmem, vmem),
        scratch_shapes=[
            *[pltpu.VMEM(operand.shape, operand.dtype) for operand in operands],
            pltpu.VMEM((channels // LANES, LANES, 2 * LANES), jnp.bfloat16),
            pltpu.VMEM((tokens + TILE, channels), jnp.float32),
            pltpu.VMEM((RIM, channels), jnp.bfloat16),
            wide,
            wide,
            wide,
            pltpu.VMEM((sp_size, TILE, channels), jnp.float32),
            pltpu.VMEM((far_size, steps, rows_dev, step), jnp.bfloat16),
            pltpu.VMEM((far_size, steps, rows_dev, step), jnp.bfloat16),
            pltpu.VMEM((far_slots, steps, rows_dev, step), jnp.bfloat16),
            pltpu.VMEM((far_slots, steps, rows_dev, step), jnp.bfloat16),
            pltpu.VMEM((rows_dev, width), jnp.float32),
            pltpu.SemaphoreType.DMA((len(operands),)),
            pltpu.SemaphoreType.DMA((2,)),
            pltpu.SemaphoreType.DMA((sp_size,)),
            pltpu.SemaphoreType.DMA((sp_size,)),
            pltpu.SemaphoreType.DMA((far_size, steps)),
            pltpu.SemaphoreType.DMA((far_size, steps)),
            pltpu.SemaphoreType.DMA((far_slots, steps)),
            pltpu.SemaphoreType.DMA((far_slots, steps)),
        ],
        compiler_params=pltpu.CompilerParams(
            collective_id=0, has_side_effects=True, vmem_limit_bytes=67043328
        ),
    )(*operands)


def slot_numbers(picks, experts):
    flat = picks.reshape(-1)
    onehot = (flat[:, None] == jnp.arange(experts, dtype=jnp.int32)[None, :]).astype(jnp.int32)
    before = jnp.cumsum(onehot, axis=0) - onehot
    return (flat, jnp.sum(before * onehot, axis=1))


def fill_slots(source_rows, slot_of, row_of, slot_count):
    match = slot_of[None, :] == jnp.arange(slot_count, dtype=jnp.int32)[:, None]
    picked = jnp.sum(jnp.where(match, row_of[None, :], 0), axis=1)
    present = jnp.any(match, axis=1)
    return jnp.where(present[:, None], source_rows[picked], jnp.zeros((), source_rows.dtype))


def expert_hidden(rows, gate_weight, up_weight):
    gate = jnp.dot(rows, gate_weight[0], preferred_element_type=jnp.float32)
    upward = jnp.dot(rows, up_weight[0], preferred_element_type=jnp.float32)
    return (jax.nn.silu(gate) * upward).astype(jnp.bfloat16)


def expert_down(active, down_weight):
    columns = down_weight[0]
    return jnp.dot(
        lax.all_gather(active, "tp", axis=1, tiled=True),
        columns,
        preferred_element_type=jnp.float32,
    ).astype(jnp.bfloat16)


def phase(name):
    return contextlib.nullcontext()


def layer_kernel(
    sp_size,
    tp_size,
    capacity,
    x_hbm,
    out_gate_hbm,
    taps_hbm,
    recur_map_hbm,
    input_map_hbm,
    decay_hbm,
    boost_hbm,
    routes_hbm,
    pair_weight_hbm,
    weight_hbm,
    resid_hbm,
    gain_hbm,
    gate_hbm,
    up_hbm,
    down_hbm,
    out_ref,
    x_ref,
    out_gate_ref,
    taps_ref,
    recur_map_ref,
    input_map_ref,
    decay_ref,
    boost_ref,
    routes_ref,
    pair_weight_ref,
    weight_ref,
    resid_ref,
    gain_ref,
    gate,
    up,
    down,
    gates_ref,
    ext,
    rim,
    running,
    local,
    lifted,
    branch,
    totals,
    across,
    along,
    send_pair,
    recv_pair,
    send_far,
    recv_far,
    summed,
    stream_ref,
    normed_ref,
    other_normed,
    mirrored,
    own_weights,
    pair_weights,
    ranks,
    choose,
    choose_other,
    choose_mirror,
    mixers,
    outgoing,
    outgoing_other,
    outgoing_mirror,
    rows,
    active,
    result,
    returned,
    blend,
    gathered,
    gate_extra,
    up_extra,
    load_sems,
    rim_sems,
    extra_send,
    extra_recv,
    total_send,
    total_recv,
    pair_send,
    pair_recv,
    far_send,
    far_recv,
    cross_send,
    cross_recv,
    mirror_send,
    mirror_recv,
    route_sems,
    weight_send,
    weight_recv,
    out_send,
    out_recv,
    near_send,
    near_recv,
    pass_send,
    pass_recv,
    row_far_send,
    row_far_recv,
    row_pair_send,
    row_pair_recv,
    half_send,
    half_recv,
    half_pair_send,
    half_pair_recv,
    back_half_send,
    back_half_recv,
    blend_send,
    blend_recv,
    store_sems,
):
    sp, tp = lax.axis_index("sp"), lax.axis_index("tp")
    tokens, channels = x_ref.shape
    taps = taps_ref.shape[0]
    rows_dev, width = resid_ref.shape
    picks = routes_ref.shape[1]
    hidden, columns = gate.shape[1], down.shape[1]
    core, far = lax.rem(tp, 2), tp // 2
    other = 1 - far
    partner = far * 2 + 1 - core
    across_tp = other * 2 + core
    half = sp_size // 2
    steps, step = send_pair.shape[1], send_pair.shape[3]
    kept = hidden - gate_extra.shape[1]
    pieces = far_send.shape[0]
    piece = rows_dev // pieces

    def flipped(d):
        total, bit = 0, 1
        while bit < sp_size:
            total = total + bit * lax.rem(sp // bit + d // bit, 2)
            bit *= 2
        return total

    sources = (
        (x_hbm, x_ref),
        (out_gate_hbm, out_gate_ref),
        (taps_hbm, taps_ref),
        (recur_map_hbm, recur_map_ref),
        (input_map_hbm, input_map_ref),
        (decay_hbm, decay_ref),
        (boost_hbm, boost_ref),
        (routes_hbm, routes_ref.at[0:tp_size]),
        (pair_weight_hbm, pair_weight_ref),
        (weight_hbm, weight_ref),
        (resid_hbm, resid_ref),
        (gain_hbm, gain_ref),
        (gate_hbm.at[0], gate),
        (up_hbm.at[0], up),
        (down_hbm.at[0], down),
    )
    loads = [
        pltpu.make_async_copy(source, target, load_sems.at[n])
        for n, (source, target) in enumerate(sources)
    ]
    for load in loads[:12]:
        load.start()

    barrier = pltpu.get_barrier_semaphore()
    for d in range(1, sp_size):
        pl.semaphore_signal(barrier, inc=1, **at_device(lax.rem(sp + d, sp_size), tp))
    for u in range(1, tp_size):
        pl.semaphore_signal(barrier, inc=1, **at_device(sp, lax.rem(tp + u, tp_size)))

    loads[0].wait()
    chunks = tokens // CHUNK

    @pl.loop(0, chunks)
    def _(i):
        r = pl.multiple_of(i * CHUNK, CHUNK)
        ext[pl.ds(r + TILE, CHUNK), :] = x_ref[pl.ds(r, CHUNK), :].astype(jnp.float32)

    for load in loads[2:6]:
        load.wait()
    map_size = recur_map_ref.shape[1]
    per = LANES // map_size
    gates_ref[...] = jnp.zeros_like(gates_ref)
    for b in range(channels // LANES):
        for n in range(per):
            spots = slice(n * map_size, (n + 1) * map_size)
            for side, maps in enumerate((recur_map_ref, input_map_ref)):
                start = side * LANES + n * map_size
                gates_ref[b, spots, start : start + map_size] = maps[b * per + n]
    raw = decay_ref[...]
    small = jnp.exp(-jnp.abs(raw))
    series = small * (1 - small * (1 / 2 - small * (1 / 3 - small * (1 / 4 - small * (1 / 5 - small / 6)))))
    plus = jnp.maximum(-raw, 0.0) + jnp.where(small < 0.05, series, jnp.log(1.0 + small))
    scale = -RECURRENT_SCALE * plus

    loads[8].wait()
    own_weights[...] = jnp.zeros_like(own_weights)
    own_weights[0:picks, :] = pair_weight_ref[...]
    pair_weights[tp] = own_weights[...]

    with phase("barrier"):
        pl.semaphore_wait(barrier, sp_size - 1 + tp_size - 1)
    rim_copy = pltpu.make_async_remote_copy(
        src_ref=x_ref.at[pl.ds(tokens - RIM, RIM)],
        dst_ref=rim,
        send_sem=rim_sems.at[0],
        recv_sem=rim_sems.at[1],
        **at_device(lax.rem(sp + 1, sp_size), tp),
    )
    rim_copy.start()

    def extra_copy(n):
        source, target = ((gate_hbm, gate_extra), (up_hbm, up_extra))[n]
        return pltpu.make_async_remote_copy(
            src_ref=source.at[0, :, kept:hidden],
            dst_ref=target,
            send_sem=extra_send.at[n],
            recv_sem=extra_recv.at[n],
            **at_device(sp, across_tp),
        )

    @pl.when(core == 0)
    def _():
        for n in range(2):
            extra_copy(n).start()

    def weight_copy(u):
        return pltpu.make_async_remote_copy(
            src_ref=own_weights,
            dst_ref=pair_weights.at[tp],
            send_sem=weight_send.at[u],
            recv_sem=weight_recv.at[u],
            **at_device(sp, lax.rem(tp + u, tp_size)),
        )

    for u in range(1, tp_size):
        weight_copy(u).start()
    loads[7].wait()
    route_copy = pltpu.make_async_remote_copy(
        src_ref=routes_ref.at[tp],
        dst_ref=routes_ref.at[tp_size],
        send_sem=route_sems.at[0],
        recv_sem=route_sems.at[1],
        **at_device(flipped(half), tp),
    )
    route_copy.start()
    loads[6].wait()
    for load in loads[12:]:
        load.start()

    tile_row = lax.broadcasted_iota(jnp.int32, (CHUNK, LANES), 0) % TILE

    def chunk(i, carry):
        r = pl.multiple_of(i * CHUNK, CHUNK)
        out = []
        for b in range(channels // LANES):
            cols = slice(b * LANES, (b + 1) * LANES)
            win = ext[pl.ds(r, CHUNK + TILE), cols]
            base = TILE - taps + 1
            mixed = win[base : base + CHUNK] * taps_ref[0:1, cols]
            for k in range(1, taps):
                mixed = mixed + win[base + k : base + k + CHUNK] * taps_ref[k : k + 1, cols]
            smoothed = mixed.astype(jnp.bfloat16)
            both = jnp.dot(smoothed, gates_ref[b], preferred_element_type=jnp.float32)
            recur = jax.nn.sigmoid(both[:, :LANES])
            inward = jax.nn.sigmoid(both[:, LANES:])
            log_decay = recur * scale[0:1, cols] + boost_ref[pl.ds(r, CHUNK), cols]
            a = jnp.exp(log_decay)
            h = jnp.sqrt(one_minus_exp(2.0 * log_decay)) * (inward * smoothed.astype(jnp.float32))
            for s in (1, 2, 4):
                inside = tile_row >= s
                a_before = jnp.where(inside, pltpu.roll(a, s, 0), 1.0)
                h_before = jnp.where(inside, pltpu.roll(h, s, 0), 0.0)
                h = a * h_before + h
                a = a * a_before
            carry_a, carry_h = carry[2 * b], carry[2 * b + 1]
            for t in range(CHUNK // TILE):
                spots = slice(t * TILE, (t + 1) * TILE)
                h_t = h[spots] + a[spots] * carry_h
                a_t = a[spots] * carry_a
                running[pl.ds(r + t * TILE, TILE), cols] = a_t
                local[pl.ds(r + t * TILE, TILE), cols] = h_t
                carry_a, carry_h = a_t[TILE - 1 : TILE], h_t[TILE - 1 : TILE]
            out += [carry_a, carry_h]
        return tuple(out)

    ones, zeros = jnp.ones((1, LANES), jnp.float32), jnp.zeros((1, LANES), jnp.float32)
    start = (ones, zeros) * (channels // LANES)
    with phase("scan"):
        rest = lax.fori_loop(1, chunks, chunk, start)
    with phase("rim"):
        rim_copy.wait()
    edge = rim[...].astype(jnp.float32)[RIM - TILE :, :]
    ext[0:TILE, :] = jnp.where(sp == 0, 0.0, edge)
    with phase("head"):
        first = lax.fori_loop(0, 1, chunk, start)
    pick = lax.broadcasted_iota(jnp.int32, (TILE, LANES), 0) == 0
    for b in range(channels // LANES):
        first_a, first_h, rest_a, rest_h = first[2 * b], first[2 * b + 1], rest[2 * b], rest[2 * b + 1]
        totals[sp, :, b * LANES : (b + 1) * LANES] = jnp.where(
            pick, first_a * rest_a, rest_a * first_h + rest_h
        )
    head_a = jnp.concatenate(first[0::2], axis=1)
    head_h = jnp.concatenate(first[1::2], axis=1)

    total_copies = []
    for d in range(1, sp_size):
        copy = pltpu.make_async_remote_copy(
            src_ref=totals.at[sp],
            dst_ref=totals.at[sp],
            send_sem=total_send.at[d],
            recv_sem=total_recv.at[d],
            **at_device(lax.rem(sp + d, sp_size), tp),
        )
        copy.start()
        total_copies.append(copy)

    loads[1].wait()

    with phase("gelu"):

        @pl.loop(0, chunks)
        def _(i):
            r = pl.multiple_of(i * CHUNK, CHUNK)
            lifted[pl.ds(r, CHUNK), :] = jax.nn.gelu(
                out_gate_ref[pl.ds(r, CHUNK), :].astype(jnp.float32)
            )

    for load in loads[9:12]:
        load.wait()
    with phase("totals"):
        for copy in total_copies:
            copy.wait()

    entering = jnp.zeros((1, channels), jnp.float32)
    for k in range(sp_size):
        part = totals[k]
        after = part[0:1] * entering + part[1:2]
        entering = jnp.where(k < sp, after, entering)
    entering_rest = head_a * entering + head_h

    both_rows = 2 * rows_dev

    def fill_branch(side):
        for q in range(both_rows // CHUNK):
            r = pl.multiple_of(side * both_rows + q * CHUNK, CHUNK)
            at = pl.ds(r, CHUNK)
            before = entering_rest
            if q == 0:
                before = jnp.where(side == 0, entering, entering_rest)
            state = local[at, :] + running[at, :] * before
            branch[at, :] = (lifted[at, :] * state).astype(jnp.bfloat16)

    def pair_copy(k, n):
        return pltpu.make_async_remote_copy(
            src_ref=send_pair.at[k, n],
            dst_ref=recv_pair.at[k, n],
            send_sem=pair_send.at[k, n],
            recv_sem=pair_recv.at[k, n],
            **at_device(sp, partner),
        )

    def project(side, target, k, send):
        fill_branch(side)
        given = branch[pl.ds(pl.multiple_of(side * both_rows, both_rows), both_rows), :]
        for n in range(steps):
            cols = slice(n * step, (n + 1) * step)
            product = jnp.dot(given, weight_ref[:, cols], preferred_element_type=jnp.float32)
            target[0, :, cols] = product[:rows_dev]
            target[1, :, cols] = product[rows_dev:]
            send_pair[k, n] = target[1 - core, :, cols].astype(jnp.bfloat16)
            if send:
                pair_copy(k, n).start()

    with phase("project"):
        project(other, across, 0, True)
        project(far, along, 1, False)

    def far_copy(q):
        return pltpu.make_async_remote_copy(
            src_ref=send_far.at[pl.ds(q * piece, piece)],
            dst_ref=recv_far.at[pl.ds(q * piece, piece)],
            send_sem=far_send.at[q],
            recv_sem=far_recv.at[q],
            **at_device(sp, across_tp),
        )

    with phase("far_send"):
        for n in range(steps):
            pair_copy(0, n).wait_recv()
        for q in range(pieces):
            at = slice(q * piece, (q + 1) * piece)
            for n in range(steps):
                cols = slice(n * step, (n + 1) * step)
                sum_far = across[core, at, cols] + recv_pair[0, n, at, :].astype(jnp.float32)
                send_far[at, cols] = sum_far.astype(jnp.bfloat16)
            far_copy(q).start()
    for n in range(steps):
        pair_copy(1, n).start()
    for n in range(steps):
        cols = slice(n * step, (n + 1) * step)
        pair_copy(1, n).wait_recv()
        summed[:, cols] = (
            along[core, :, cols]
            + resid_ref[:, cols].astype(jnp.float32)
            + recv_pair[1, n].astype(jnp.float32)
        )

    slot_row = lax.broadcasted_iota(jnp.int32, (capacity, rows_dev), 0)
    expert_row = lax.broadcasted_iota(jnp.int32, (sp_size, rows_dev), 0)
    earlier = lax.broadcasted_iota(jnp.int32, (rows_dev, rows_dev), 0) < lax.broadcasted_iota(
        jnp.int32, (rows_dev, rows_dev), 1
    )
    earlier = jnp.where(earlier, 1.0, 0.0).astype(jnp.bfloat16)

    route_copy.wait()

    @pl.loop(0, tp_size + 1)
    def _(block):
        chosen = routes_ref[block]
        hits = jnp.zeros((sp_size, rows_dev), jnp.float32)
        for k in range(picks):
            hits = hits + jnp.where(expert_row == chosen[k : k + 1], 1.0, 0.0)
        ranks[block] = jnp.dot(hits.astype(jnp.bfloat16), earlier, preferred_element_type=jnp.float32)

    def selector(block, expert, values):
        chosen = routes_ref[block]
        value = jnp.zeros((1, rows_dev), jnp.float32)
        for k in range(picks):
            value = value + jnp.where(chosen[k : k + 1] == expert, values[k : k + 1], 0.0)
        rank = ranks[block, pl.ds(expert, 1), :].astype(jnp.int32)
        return jnp.where(rank == slot_row, value, 0.0)

    def slot_rows(block):
        return pl.ds(pl.multiple_of(block * capacity, capacity), capacity)

    unit = jnp.ones((picks, rows_dev), jnp.float32)

    @pl.loop(0, half)
    def _(d):
        expert = flipped(d)
        choose[slot_rows(d), :] = selector(tp, expert, unit).astype(jnp.bfloat16)
        choose_other[slot_rows(d), :] = selector(across_tp, expert, unit).astype(jnp.bfloat16)
        choose_mirror[slot_rows(d), :] = selector(tp_size, expert, unit).astype(jnp.bfloat16)

    with phase("weights"):
        for u in range(1, tp_size):
            weight_copy(u).wait_recv()

    with phase("mixers"):

        @pl.loop(0, tp_size)
        def _(block):
            weight = pair_weights[block]
            coarse = weight.astype(jnp.bfloat16).astype(jnp.float32)
            for n, values in enumerate((coarse, weight - coarse)):
                picked = [selector(block, e, values) for e in range(sp_size)]
                mixers[block, n] = jnp.concatenate(picked, axis=0).T.astype(jnp.bfloat16)

    def cross_copy(q):
        return pltpu.make_async_remote_copy(
            src_ref=normed_ref.at[pl.ds(q * piece, piece)],
            dst_ref=other_normed.at[pl.ds(q * piece, piece)],
            send_sem=cross_send.at[q],
            recv_sem=cross_recv.at[q],
            **at_device(sp, across_tp),
        )

    def mirror_copy(q):
        return pltpu.make_async_remote_copy(
            src_ref=normed_ref.at[pl.ds(q * piece, piece)],
            dst_ref=mirrored.at[pl.ds(q * piece, piece)],
            send_sem=mirror_send.at[q],
            recv_sem=mirror_recv.at[q],
            **at_device(flipped(half), tp),
        )

    with phase("norm"):
        for q in range(pieces):
            at = slice(q * piece, (q + 1) * piece)
            far_copy(q).wait_recv()
            squares = jnp.zeros((piece, 1), jnp.float32)
            for n in range(steps):
                cols = slice(n * step, (n + 1) * step)
                stream = (summed[at, cols] + recv_far[at, cols].astype(jnp.float32)).astype(jnp.bfloat16)
                stream_ref[at, cols] = stream
                wide = stream.astype(jnp.float32)
                squares = squares + jnp.sum(wide * wide, axis=1, keepdims=True)
            norm = lax.rsqrt(squares * (1.0 / width) + EPSILON)
            for n in range(steps):
                cols = slice(n * step, (n + 1) * step)
                wide = stream_ref[at, cols].astype(jnp.float32)
                normed_ref[at, cols] = (wide * norm * gain_ref[0:1, cols]).astype(jnp.bfloat16)
            cross_copy(q).start()
            mirror_copy(q).start()

    def out_copy(d):
        return pltpu.make_async_remote_copy(
            src_ref=outgoing.at[slot_rows(d)],
            dst_ref=rows.at[sp, slot_rows(tp)],
            send_sem=out_send.at[d],
            recv_sem=out_recv.at[d],
            **at_device(flipped(d), tp),
        )

    def near_copy(d):
        return pltpu.make_async_remote_copy(
            src_ref=outgoing_other.at[slot_rows(d)],
            dst_ref=rows.at[sp, slot_rows(across_tp)],
            send_sem=near_send.at[d],
            recv_sem=near_recv.at[d],
            **at_device(flipped(d), tp),
        )

    def pass_copy(e):
        return pltpu.make_async_remote_copy(
            src_ref=outgoing_mirror.at[slot_rows(e)],
            dst_ref=rows.at[flipped(half), slot_rows(tp)],
            send_sem=pass_send.at[e],
            recv_sem=pass_recv.at[e],
            **at_device(flipped(e), tp),
        )

    def row_far(d):
        place = rows.at[flipped(d), slot_rows(tp)]
        return pltpu.make_async_remote_copy(
            src_ref=place,
            dst_ref=place,
            send_sem=row_far_send.at[d - half],
            recv_sem=row_far_recv.at[d - half],
            **at_device(sp, across_tp),
        )

    def row_pair(d, j):
        place = rows.at[flipped(d), slot_rows(across_tp if j else tp)]
        return pltpu.make_async_remote_copy(
            src_ref=place,
            dst_ref=place,
            send_sem=row_pair_send.at[d, j],
            recv_sem=row_pair_recv.at[d, j],
            **at_device(sp, partner),
        )

    half_slots = 2 * capacity

    def side_rows(side):
        return pl.ds(pl.multiple_of(side * half_slots, half_slots), half_slots)

    sides = (far, other)

    def half_copy(d, h, end):
        place = active.at[flipped(d), tp, side_rows(sides[h]), 0:end]
        return pltpu.make_async_remote_copy(
            src_ref=place,
            dst_ref=place,
            send_sem=half_send.at[d, h],
            recv_sem=half_recv.at[d, h],
            **at_device(sp, across_tp),
        )

    def on_half(d, h, act):
        @pl.when(core == 0)
        def _():
            act(half_copy(d, h, kept))

        @pl.when(core == 1)
        def _():
            act(half_copy(d, h, hidden))

    def half_start(d, h):
        on_half(d, h, lambda copy: copy.start())

    def half_pair(d, j, h):
        place = active.at[flipped(d), across_tp if j else tp, side_rows(sides[h])]
        return pltpu.make_async_remote_copy(
            src_ref=place,
            dst_ref=place,
            send_sem=half_pair_send.at[d, 2 * j + h],
            recv_sem=half_pair_recv.at[d, 2 * j + h],
            **at_device(sp, partner),
        )

    def back_half(d, h):
        return pltpu.make_async_remote_copy(
            src_ref=result.at[d, side_rows(sides[h])],
            dst_ref=returned.at[sp, side_rows(sides[h])],
            send_sem=back_half_send.at[d, h],
            recv_sem=back_half_recv.at[d, h],
            **at_device(flipped(d), tp),
        )

    mates = (across_tp, other * 2 + 1 - core, partner)

    def blend_copy(u):
        return pltpu.make_async_remote_copy(
            src_ref=blend.at[u],
            dst_ref=gathered.at[tp],
            send_sem=blend_send.at[u],
            recv_sem=blend_recv.at[u],
            **at_device(sp, mates[u]),
        )

    pack_rows = half * capacity

    def pack(chooser, given, target):
        for n in range(steps):
            cols = slice(n * step, (n + 1) * step)
            target[:, cols] = jnp.dot(
                chooser[...], given[:, cols], preferred_element_type=jnp.float32
            ).astype(jnp.bfloat16)

    def hidden_part(given, gate_part, up_part):
        gated = jnp.dot(given, gate_part[...], preferred_element_type=jnp.float32)
        upward = jnp.dot(given, up_part[...], preferred_element_type=jnp.float32)
        return (jax.nn.silu(gated) * upward).astype(jnp.bfloat16)

    def fill_hidden(d, h):
        source = flipped(d)
        at = side_rows(sides[h])
        active[source, tp, at, :] = hidden_part(rows[source, at, :], gate, up)
        half_pair(d, 0, h).start()

    def fill_extra(d, h):
        source = flipped(d)
        at = side_rows(sides[h])

        @pl.when(core == 0)
        def _():
            active[source, across_tp, at, kept:hidden] = hidden_part(
                rows[source, at, :], gate_extra, up_extra
            )

    def first(d):
        with phase("w_first"):
            row_pair(d, 0).wait_recv()
        fill_hidden(d, 0)
        half_start(d, 0)
        fill_extra(d, 0)

    def second(d):
        with phase("w_second"):
            row_pair(d, 1).wait_recv()
        fill_hidden(d, 1)
        fill_extra(d, 1)

    def relay(d, h):
        with phase("w_relay"):
            on_half(d, h, lambda copy: copy.wait_recv())
        half_pair(d, 1, 1 - h).start()

    def down_side(d, h):
        with phase("w_down"):
            half_pair(d, 0, h).wait_recv()
            half_pair(d, 1, h).wait_recv()
        source = flipped(d)
        at = side_rows(sides[h])
        total = jnp.dot(active[source, 0, at, :], down[0:hidden, :], preferred_element_type=jnp.float32)
        for t in range(1, tp_size):
            total = total + jnp.dot(
                active[source, t, at, :],
                down[t * hidden : (t + 1) * hidden, :],
                preferred_element_type=jnp.float32,
            )
        made = total.astype(jnp.bfloat16)
        result[d, at, :] = made

        @pl.when(d == 0)
        def _():
            returned[sp, at, :] = made

        @pl.when(d > 0)
        def _():
            back_half(d, h).start()

    def near_first(d):
        with phase("w_own"):

            @pl.when(d > 0)
            def _():
                out_copy(d).wait_recv()
                row_pair(d, 0).start()

        first(d)

    def near_arrived(d):
        with phase("w_near"):

            @pl.when(d > 0)
            def _():
                near_copy(d).wait_recv()
                row_pair(d, 1).start()

    with phase("pack"):
        pack(choose, normed_ref, outgoing)
        out_copy(1).start()
        rows[sp, slot_rows(tp), :] = outgoing[0:capacity, :]
        row_pair(0, 0).start()
    for load in loads[12:]:
        load.wait()

    @pl.when(core == 0)
    def _():
        for n in range(2):
            extra_copy(n).wait_recv()

    @pl.loop(0, half // 2)
    def _(d):
        near_first(d)

    with phase("cross"):
        for q in range(pieces):
            cross_copy(q).wait_recv()
    with phase("pack_other"):
        pack(choose_other, other_normed, outgoing_other)
        rows[sp, slot_rows(across_tp), :] = outgoing_other[0:capacity, :]
        row_pair(0, 1).start()
    with phase("mirror"):
        for q in range(pieces):
            mirror_copy(q).wait_recv()
    with phase("pack_mirror"):
        pack(choose_mirror, mirrored, outgoing_mirror)
        for e in range(1, min(3, half)):
            pass_copy(e).start()
        near_copy(1).start()
        rows[flipped(half), slot_rows(tp), :] = outgoing_mirror[0:capacity, :]
        row_far(half).start()
        row_pair(half, 0).start()

    first(half)

    @pl.loop(1, half + 1)
    def _(s):
        d = half + s
        near = s - 1

        @pl.when(s < half)
        def _():
            with phase("w_pass"):
                pass_copy(s).wait_recv()
            row_far(d).start()
            row_pair(d, 0).start()

        @pl.when(s + 2 < half)
        def _():
            pass_copy(s + 2).start()

        @pl.when(s + 1 < half)
        def _():
            out_copy(s + 1).start()
            near_copy(s + 1).start()

        with phase("w_rowfar"):
            row_far(d - 1).wait_recv()
        row_pair(d - 1, 1).start()

        @pl.when(s >= 2)
        def _():
            relay(d - 2, 1)

        @pl.when(s < half)
        def _():
            first(d)

        second(d - 1)
        half_start(d - 1, 1)
        relay(d - 1, 0)
        near_arrived(near)

        @pl.when(s >= 2)
        def _():
            down_side(d - 2, 0)

        @pl.when(near >= half // 2)
        def _():
            near_first(near)

        down_side(d - 1, 1)

        second(near)

        @pl.when(near < half // 2)
        def _():
            relay(near, 0)
            down_side(near, 1)

    for d in reversed(range(half)):
        half_start(d, 1)

    relay(sp_size - 1, 1)

    @pl.loop(half // 2, half)
    def _(d):
        relay(d, 0)
        down_side(d, 1)

    down_side(sp_size - 1, 0)

    @pl.loop(1, half)
    def _(d):
        relay(half - d, 1)

    @pl.loop(1, half)
    def _(d):
        down_side(half - d, 0)

    def blended(block):
        part = returned[:, slot_rows(block), :].reshape(sp_size * capacity, columns)
        total = jnp.dot(mixers[block, 0], part, preferred_element_type=jnp.float32)
        total = total + jnp.dot(mixers[block, 1], part, preferred_element_type=jnp.float32)
        return total.astype(jnp.bfloat16)

    with phase("w_back"):

        @pl.loop(1, sp_size)
        def _(d):
            back_half(d, 1).wait_recv()

    with phase("blend"):
        for u in range(2):
            blend[u] = blended(mates[u])
            blend_copy(u).start()

    relay(0, 1)
    down_side(0, 0)

    @pl.loop(1, sp_size)
    def _(d):
        back_half(d, 0).wait_recv()

    blend[2] = blended(partner)
    blend_copy(2).start()
    gathered[tp] = blended(tp)
    def finish(n, t):
        cols = pl.ds(pl.multiple_of(t * columns, columns), columns)
        normed_ref[:, cols] = (
            stream_ref[:, cols].astype(jnp.float32) + gathered[t].astype(jnp.float32)
        ).astype(jnp.bfloat16)
        pltpu.make_async_copy(normed_ref.at[:, cols], out_ref.at[:, cols], store_sems.at[n]).start()

    for k in range(2):
        for n in range(steps):
            pair_copy(k, n).wait_send()
    for q in range(pieces):
        far_copy(q).wait_send()
        cross_copy(q).wait_send()
        mirror_copy(q).wait_send()
    for u in range(1, tp_size):
        weight_copy(u).wait_send()

    @pl.when(core == 0)
    def _():
        for n in range(2):
            extra_copy(n).wait_send()


    @pl.loop(1, half)
    def _(d):
        out_copy(d).wait_send()
        near_copy(d).wait_send()
        pass_copy(d).wait_send()

    @pl.loop(1, sp_size)
    def _(d):
        for h in range(2):
            back_half(d, h).wait_send()

    @pl.loop(half, sp_size)
    def _(d):
        row_far(d).wait_send()

    @pl.loop(0, sp_size)
    def _(d):
        for h in range(2):
            row_pair(d, h).wait_send()
            on_half(d, h, lambda copy: copy.wait_send())
            for j in range(2):
                half_pair(d, j, h).wait_send()

    finish(0, tp)
    for n, u in enumerate((2, 0, 1)):
        with phase("w_blend"):
            blend_copy(u).wait_recv()
        finish(n + 1, mates[u])
    for u in range(tp_size - 1):
        blend_copy(u).wait_send()
    for n, t in enumerate((tp, mates[2], mates[0], mates[1])):
        cols = pl.ds(pl.multiple_of(t * columns, columns), columns)
        pltpu.make_async_copy(normed_ref.at[:, cols], out_ref.at[:, cols], store_sems.at[n]).wait()


def fused_layer(
    resid,
    recurrent_input,
    recurrent_out_gate,
    filter_weight,
    recurrence_gate_matrix,
    input_gate_matrix,
    channel_decay_raw,
    token_decay_boost,
    output_projection_weight,
    expert_norm_gain,
    routes,
    expert_pair_weight,
    gate_weight,
    up_weight,
    down_weight,
    capacity,
):
    sp_size, tp_size = lax.axis_size("sp"), lax.axis_size("tp")
    tokens, channels = recurrent_input.shape
    rows_dev, width = resid.shape
    hidden, columns = gate_weight.shape[2], down_weight.shape[2]
    step = 512 if width % 512 == 0 else width
    steps = width // step
    pieces = 4 if rows_dev % (4 * RIM) == 0 else 1
    half = sp_size // 2
    slots_all = tp_size * capacity
    narrow = (
        recurrent_input,
        recurrent_out_gate,
        filter_weight,
        recurrence_gate_matrix,
        input_gate_matrix,
        channel_decay_raw.reshape(1, channels),
        token_decay_boost,
        routes.reshape(tp_size, rows_dev, -1).swapaxes(1, 2),
        expert_pair_weight.T,
        output_projection_weight,
        resid,
        expert_norm_gain.reshape(1, width),
    )
    operands = (*narrow, gate_weight, up_weight, down_weight)
    dma = pltpu.SemaphoreType.DMA

    def buffer(*shape):
        return pltpu.VMEM(shape, jnp.bfloat16)

    def wide(*shape):
        return pltpu.VMEM(shape, jnp.float32)

    return pl.pallas_call(
        functools.partial(layer_kernel, sp_size, tp_size, capacity),
        out_shape=jax.ShapeDtypeStruct((rows_dev, width), jnp.bfloat16),
        in_specs=[pl.BlockSpec(memory_space=pltpu.HBM)] * len(operands),
        out_specs=pl.BlockSpec(memory_space=pltpu.HBM),
        scratch_shapes=[
            *[pltpu.VMEM(operand.shape, operand.dtype) for operand in narrow[:7]],
            pltpu.VMEM((tp_size + 1, *narrow[7].shape[1:]), narrow[7].dtype),
            *[pltpu.VMEM(operand.shape, operand.dtype) for operand in narrow[8:]],
            buffer(*gate_weight.shape[1:]),
            buffer(*up_weight.shape[1:]),
            buffer(*down_weight.shape[1:]),
            buffer(channels // LANES, LANES, 2 * LANES),
            wide(tokens + TILE, channels),
            buffer(RIM, channels),
            wide(tokens, channels),
            wide(tokens, channels),
            wide(tokens, channels),
            buffer(tokens, channels),
            wide(sp_size, TILE, channels),
            wide(2, rows_dev, width),
            wide(2, rows_dev, width),
            buffer(2, steps, rows_dev, step),
            buffer(2, steps, rows_dev, step),
            buffer(rows_dev, width),
            buffer(rows_dev, width),
            wide(rows_dev, width),
            buffer(rows_dev, width),
            buffer(rows_dev, width),
            buffer(rows_dev, width),
            buffer(rows_dev, width),
            wide(TILE, rows_dev),
            wide(tp_size, TILE, rows_dev),
            wide(tp_size + 1, sp_size, rows_dev),
            *[buffer(half * capacity, rows_dev)] * 3,
            buffer(tp_size, 2, rows_dev, sp_size * capacity),
            *[buffer(half * capacity, width)] * 3,
            buffer(sp_size, slots_all, width),
            buffer(sp_size, tp_size, slots_all, hidden),
            buffer(sp_size, slots_all, columns),
            buffer(sp_size, slots_all, columns),
            buffer(tp_size - 1, rows_dev, columns),
            buffer(tp_size, rows_dev, columns),
            buffer(width, LANES),
            buffer(width, LANES),
            dma((len(operands),)),
            dma((2,)),
            dma((2,)),
            dma((2,)),
            dma((sp_size,)),
            dma((sp_size,)),
            dma((2, steps)),
            dma((2, steps)),
            *[dma((pieces,))] * 6,
            dma((2,)),
            dma((tp_size,)),
            dma((tp_size,)),
            *[dma((half,))] * 8,
            *[dma((sp_size, 2))] * 4,
            dma((sp_size, 4)),
            dma((sp_size, 4)),
            dma((sp_size, 2)),
            dma((sp_size, 2)),
            dma((tp_size - 1,)),
            dma((tp_size - 1,)),
            dma((tp_size,)),
        ],
        compiler_params=pltpu.CompilerParams(
            collective_id=1, has_side_effects=True, vmem_limit_bytes=58720256
        ),
    )(*operands)


def body(
    resid,
    recurrent_input,
    recurrent_out_gate,
    filter_weight,
    recurrence_gate_matrix,
    input_gate_matrix,
    channel_decay_raw,
    token_decay_boost,
    output_projection_weight,
    expert_norm_gain,
    routes,
    expert_pair_weight,
    gate_weight,
    up_weight,
    down_weight,
):
    tp_size = lax.axis_size("tp")
    experts = lax.axis_size("sp")
    rows_dev, model_width = resid.shape
    capacity = max(2, 3 * rows_dev // experts)
    fits = capacity % RIM == 0 and rows_dev % LANES == 0
    fits = fits and gate_weight.shape[2] % LANES == 0 and gate_weight.shape[2] > LANES
    if fits and tp_size == 4 and experts >= 4 and experts & (experts - 1) == 0:
        return fused_layer(
            resid,
            recurrent_input,
            recurrent_out_gate,
            filter_weight,
            recurrence_gate_matrix,
            input_gate_matrix,
            channel_decay_raw,
            token_decay_boost,
            output_projection_weight,
            expert_norm_gain,
            routes,
            expert_pair_weight,
            gate_weight,
            up_weight,
            down_weight,
            capacity,
        )
    stream, normed = recurrence(
        resid,
        recurrent_input,
        recurrent_out_gate,
        filter_weight,
        recurrence_gate_matrix,
        input_gate_matrix,
        channel_decay_raw,
        token_decay_boost,
        output_projection_weight,
        expert_norm_gain,
    )
    stream_wide = stream.astype(jnp.float32)
    own_routes = lax.dynamic_slice_in_dim(routes, lax.axis_index("tp") * rows_dev, rows_dev, 0)
    own_flat, own_rank = slot_numbers(own_routes, experts)
    own_slots = own_flat * capacity + own_rank
    row_of = jnp.arange(2 * rows_dev, dtype=jnp.int32) // 2
    outgoing = fill_slots(normed, own_slots, row_of, experts * capacity).reshape(
        experts, capacity, model_width
    )
    arrived = lax.all_to_all(outgoing, "sp", split_axis=0, concat_axis=0, tiled=True)
    piece = lax.all_gather(
        arrived.reshape(1, experts * capacity, model_width), "tp", axis=0, tiled=True
    )
    flat_rows = piece.reshape(piece.shape[0] * piece.shape[1], model_width)
    active = expert_hidden(flat_rows, gate_weight, up_weight).reshape(
        piece.shape[0], piece.shape[1], -1
    )
    result = expert_down(active.reshape(-1, active.shape[2]), down_weight)
    joined = lax.all_to_all(
        result.reshape(tp_size, experts * capacity, -1),
        "tp",
        split_axis=0,
        concat_axis=2,
        tiled=True,
    )
    returned = lax.all_to_all(
        joined.reshape(experts, capacity, model_width),
        "sp",
        split_axis=0,
        concat_axis=0,
        tiled=True,
    )
    picked = (
        returned.reshape(experts * capacity, model_width)[own_slots]
        .astype(jnp.float32)
        .reshape(rows_dev, 2, model_width)
    )
    blended = jnp.sum(picked * expert_pair_weight[:, :, None], axis=1)
    return (stream_wide + blended).astype(jnp.bfloat16)


def solution(mesh):
    placed = (
        P(("sp", "tp"), None),
        P("sp", "tp"),
        P("sp", "tp"),
        P(None, "tp"),
        P("tp", None, None),
        P("tp", None, None),
        P("tp"),
        P("sp", "tp"),
        P("tp", None),
        P(),
        P("sp", None),
        P(("sp", "tp"), None),
        P("sp", None, "tp"),
        P("sp", None, "tp"),
        P("sp", None, "tp"),
    )
    return jax.shard_map(
        body, mesh=mesh, in_specs=placed, out_specs=P(("sp", "tp"), None), check_vma=False
    )
```

```python
import contextlib
import functools

import jax
import jax.numpy as jnp
from jax import lax
from jax.experimental import pallas as pl
from jax.experimental.pallas import tpu as pltpu
from jax.sharding import PartitionSpec as P

RECURRENT_SCALE = 8.0
EPSILON = 1e-06
LANES = 128
TILE = 8
CHUNK = 64
RIM = 16
MESH = pl.DeviceIdType.MESH


def at_device(sp, tp):
    return {"device_id": (sp, tp), "device_id_type": MESH}


def one_minus_exp(y):
    series = 1.0 + y * (1 / 2 + y * (1 / 6 + y * (1 / 24 + y * (1 / 120 + y * (1 / 720 + y / 5040)))))
    series = series * -y
    return jnp.where(y > -0.4, series, 1.0 - jnp.exp(y))


def recurrence_kernel(
    sp_size,
    tp_size,
    x_hbm,
    out_gate_hbm,
    taps_hbm,
    recur_map_hbm,
    input_map_hbm,
    decay_hbm,
    boost_hbm,
    weight_hbm,
    resid_hbm,
    gain_hbm,
    stream_ref,
    normed_ref,
    x_ref,
    out_gate_ref,
    taps_ref,
    recur_map_ref,
    input_map_ref,
    decay_ref,
    boost_ref,
    weight_ref,
    resid_ref,
    gain_ref,
    gates_ref,
    ext,
    rim,
    running,
    local,
    lifted,
    totals,
    send_pair,
    recv_pair,
    send_far,
    recv_far,
    summed,
    load_sems,
    rim_sems,
    total_send_sems,
    total_recv_sems,
    pair_send_sems,
    pair_recv_sems,
    far_send_sems,
    far_recv_sems,
):
    sp, tp = lax.axis_index("sp"), lax.axis_index("tp")
    tokens, channels = x_ref.shape
    taps = taps_ref.shape[0]
    width = weight_ref.shape[1]
    rows_dev = resid_ref.shape[0]
    far_size = tp_size // 2
    core, far = lax.rem(tp, 2), tp // 2
    partner = far * 2 + 1 - core

    sources = (
        (x_hbm, x_ref),
        (out_gate_hbm, out_gate_ref),
        (taps_hbm, taps_ref),
        (recur_map_hbm, recur_map_ref),
        (input_map_hbm, input_map_ref),
        (decay_hbm, decay_ref),
        (boost_hbm, boost_ref),
        (weight_hbm, weight_ref),
        (resid_hbm, resid_ref),
        (gain_hbm, gain_ref),
    )
    loads = [
        pltpu.make_async_copy(source, target, load_sems.at[n])
        for n, (source, target) in enumerate(sources)
    ]
    for load in loads:
        load.start()

    barrier = pltpu.get_barrier_semaphore()
    for d in range(1, sp_size):
        pl.semaphore_signal(barrier, inc=1, **at_device(lax.rem(sp + d, sp_size), tp))
    pl.semaphore_signal(barrier, inc=1, **at_device(sp, partner))
    for d in range(1, far_size):
        pl.semaphore_signal(
            barrier, inc=1, **at_device(sp, lax.rem(far + d, far_size) * 2 + core)
        )
    pl.semaphore_wait(barrier, sp_size - 1 + far_size)

    loads[0].wait()
    rim_copy = pltpu.make_async_remote_copy(
        src_ref=x_ref.at[pl.ds(tokens - RIM, RIM)],
        dst_ref=rim,
        send_sem=rim_sems.at[0],
        recv_sem=rim_sems.at[1],
        **at_device(lax.rem(sp + 1, sp_size), tp),
    )
    rim_copy.start()
    loads[1].wait()

    @pl.loop(0, tokens // CHUNK)
    def _(i):
        r = pl.multiple_of(i * CHUNK, CHUNK)
        ext[pl.ds(r + TILE, CHUNK), :] = x_ref[pl.ds(r, CHUNK), :].astype(jnp.float32)
        lifted[pl.ds(r, CHUNK), :] = jax.nn.gelu(out_gate_ref[pl.ds(r, CHUNK), :].astype(jnp.float32))

    for load in loads[2:6]:
        load.wait()
    map_size = recur_map_ref.shape[1]
    per = LANES // map_size
    gates_ref[...] = jnp.zeros_like(gates_ref)
    for b in range(channels // LANES):
        for n in range(per):
            rows = slice(n * map_size, (n + 1) * map_size)
            for side, maps in enumerate((recur_map_ref, input_map_ref)):
                start = side * LANES + n * map_size
                gates_ref[b, rows, start : start + map_size] = maps[b * per + n]
    raw = decay_ref[...]
    small = jnp.exp(-jnp.abs(raw))
    series = small * (1 - small * (1 / 2 - small * (1 / 3 - small * (1 / 4 - small * (1 / 5 - small / 6)))))
    plus = jnp.maximum(-raw, 0.0) + jnp.where(small < 0.05, series, jnp.log(1.0 + small))
    scale = -RECURRENT_SCALE * plus

    rim_copy.wait()
    loads[6].wait()
    edge = rim[...].astype(jnp.float32)[RIM - TILE :, :]
    ext[0:TILE, :] = jnp.where(sp == 0, 0.0, edge)

    tile_row = lax.broadcasted_iota(jnp.int32, (CHUNK, LANES), 0) % TILE

    def chunk(i, carry):
        r = pl.multiple_of(i * CHUNK, CHUNK)
        out = []
        for b in range(channels // LANES):
            cols = slice(b * LANES, (b + 1) * LANES)
            win = ext[pl.ds(r, CHUNK + TILE), cols]
            base = TILE - taps + 1
            mixed = win[base : base + CHUNK] * taps_ref[0:1, cols]
            for k in range(1, taps):
                mixed = mixed + win[base + k : base + k + CHUNK] * taps_ref[k : k + 1, cols]
            smoothed = mixed.astype(jnp.bfloat16)
            both = jnp.dot(smoothed, gates_ref[b], preferred_element_type=jnp.float32)
            recur = jax.nn.sigmoid(both[:, :LANES])
            inward = jax.nn.sigmoid(both[:, LANES:])
            log_decay = recur * scale[0:1, cols] + boost_ref[pl.ds(r, CHUNK), cols]
            a = jnp.exp(log_decay)
            h = jnp.sqrt(one_minus_exp(2.0 * log_decay)) * (inward * smoothed.astype(jnp.float32))
            for s in (1, 2, 4):
                inside = tile_row >= s
                a_before = jnp.where(inside, pltpu.roll(a, s, 0), 1.0)
                h_before = jnp.where(inside, pltpu.roll(h, s, 0), 0.0)
                h = a * h_before + h
                a = a * a_before
            carry_a, carry_h = carry[2 * b], carry[2 * b + 1]
            for t in range(CHUNK // TILE):
                rows = slice(t * TILE, (t + 1) * TILE)
                h_t = h[rows] + a[rows] * carry_h
                a_t = a[rows] * carry_a
                running[pl.ds(r + t * TILE, TILE), cols] = a_t
                local[pl.ds(r + t * TILE, TILE), cols] = h_t
                carry_a, carry_h = a_t[TILE - 1 : TILE], h_t[TILE - 1 : TILE]
            out += [carry_a, carry_h]
        return tuple(out)

    ones, zeros = jnp.ones((1, LANES), jnp.float32), jnp.zeros((1, LANES), jnp.float32)
    last = lax.fori_loop(0, tokens // CHUNK, chunk, (ones, zeros) * (channels // LANES))
    pick = lax.broadcasted_iota(jnp.int32, (TILE, LANES), 0) == 0
    for b in range(channels // LANES):
        totals[sp, :, b * LANES : (b + 1) * LANES] = jnp.where(pick, last[2 * b], last[2 * b + 1])

    sent = []
    for d in range(1, sp_size):
        copy = pltpu.make_async_remote_copy(
            src_ref=totals.at[sp],
            dst_ref=totals.at[sp],
            send_sem=total_send_sems.at[d],
            recv_sem=total_recv_sems.at[d],
            **at_device(lax.rem(sp + d, sp_size), tp),
        )
        copy.start()
        sent.append(copy)
    for copy in sent:
        copy.wait()

    entering = jnp.zeros((1, channels), jnp.float32)
    for k in range(sp_size):
        part = totals[k]
        after = part[0:1] * entering + part[1:2]
        entering = jnp.where(k < sp, after, entering)

    def partial_sum(block, n, step):
        rows = pl.ds(pl.multiple_of(block * rows_dev, rows_dev), rows_dev)
        state = local[rows, :] + running[rows, :] * entering
        branch = (lifted[rows, :] * state).astype(jnp.bfloat16)
        cols = slice(n * step, (n + 1) * step)
        return jnp.dot(branch, weight_ref[:, cols], preferred_element_type=jnp.float32)

    step = 512 if width % 512 == 0 else width
    steps = width // step

    for load in loads[7:]:
        load.wait()
    pair_copies = {}
    for d in range(1, far_size + 1):
        other = lax.rem(far + d, far_size)
        for n in range(steps):
            send_pair[d - 1, n] = partial_sum(other * 2 + 1 - core, n, step).astype(jnp.bfloat16)
            pair_copies[d, n] = pltpu.make_async_remote_copy(
                src_ref=send_pair.at[d - 1, n],
                dst_ref=recv_pair.at[d - 1, n],
                send_sem=pair_send_sems.at[d - 1, n],
                recv_sem=pair_recv_sems.at[d - 1, n],
                **at_device(sp, partner),
            )
            pair_copies[d, n].start()
    far_copies = {}
    for d in range(1, far_size):
        other = lax.rem(far + d, far_size)
        for n in range(steps):
            total = partial_sum(other * 2 + core, n, step)
            pair_copies[d, n].wait_recv()
            total = total + recv_pair[d - 1, n].astype(jnp.float32)
            send_far[d - 1, n] = total.astype(jnp.bfloat16)
            far_copies[d, n] = pltpu.make_async_remote_copy(
                src_ref=send_far.at[d - 1, n],
                dst_ref=recv_far.at[d - 1, n],
                send_sem=far_send_sems.at[d - 1, n],
                recv_sem=far_recv_sems.at[d - 1, n],
                **at_device(sp, other * 2 + core),
            )
            far_copies[d, n].start()

    for n in range(steps):
        cols = slice(n * step, (n + 1) * step)
        total = partial_sum(tp, n, step) + resid_ref[:, cols].astype(jnp.float32)
        pair_copies[far_size, n].wait_recv()
        summed[:, cols] = total + recv_pair[far_size - 1, n].astype(jnp.float32)

    squares = jnp.zeros((rows_dev, 1), jnp.float32)
    for n in range(steps):
        cols = slice(n * step, (n + 1) * step)
        total = summed[:, cols]
        for d in range(1, far_size):
            far_copies[d, n].wait_recv()
            total = total + recv_far[d - 1, n].astype(jnp.float32)
        stream = total.astype(jnp.bfloat16)
        stream_ref[:, cols] = stream
        wide = stream.astype(jnp.float32)
        squares = squares + jnp.sum(wide * wide, axis=1, keepdims=True)
    norm = lax.rsqrt(squares * (1.0 / width) + EPSILON)
    for n in range(steps):
        cols = slice(n * step, (n + 1) * step)
        wide = stream_ref[:, cols].astype(jnp.float32)
        normed_ref[:, cols] = (wide * norm * gain_ref[0:1, cols]).astype(jnp.bfloat16)
    for copy in [*pair_copies.values(), *far_copies.values()]:
        copy.wait_send()


def recurrence(
    resid,
    recurrent_input,
    recurrent_out_gate,
    filter_weight,
    recurrence_gate_matrix,
    input_gate_matrix,
    channel_decay_raw,
    token_decay_boost,
    output_projection_weight,
    expert_norm_gain,
):
    sp_size, tp_size = lax.axis_size("sp"), lax.axis_size("tp")
    tokens, channels = recurrent_input.shape
    rows_dev, width = resid.shape
    far_size = tp_size // 2
    step = 512 if width % 512 == 0 else width
    steps = width // step
    vmem = pl.BlockSpec(memory_space=pltpu.VMEM)
    row_shape = jax.ShapeDtypeStruct((rows_dev, width), jnp.bfloat16)
    wide = pltpu.VMEM((tokens, channels), jnp.float32)
    far_slots = max(1, far_size - 1)
    operands = (
        recurrent_input,
        recurrent_out_gate,
        filter_weight,
        recurrence_gate_matrix,
        input_gate_matrix,
        channel_decay_raw.reshape(1, channels),
        token_decay_boost,
        output_projection_weight,
        resid,
        expert_norm_gain.reshape(1, width),
    )
    return pl.pallas_call(
        functools.partial(recurrence_kernel, sp_size, tp_size),
        out_shape=(row_shape, row_shape),
        in_specs=[pl.BlockSpec(memory_space=pltpu.HBM)] * len(operands),
        out_specs=(vmem, vmem),
        scratch_shapes=[
            *[pltpu.VMEM(operand.shape, operand.dtype) for operand in operands],
            pltpu.VMEM((channels // LANES, LANES, 2 * LANES), jnp.bfloat16),
            pltpu.VMEM((tokens + TILE, channels), jnp.float32),
            pltpu.VMEM((RIM, channels), jnp.bfloat16),
            wide,
            wide,
            wide,
            pltpu.VMEM((sp_size, TILE, channels), jnp.float32),
            pltpu.VMEM((far_size, steps, rows_dev, step), jnp.bfloat16),
            pltpu.VMEM((far_size, steps, rows_dev, step), jnp.bfloat16),
            pltpu.VMEM((far_slots, steps, rows_dev, step), jnp.bfloat16),
            pltpu.VMEM((far_slots, steps, rows_dev, step), jnp.bfloat16),
            pltpu.VMEM((rows_dev, width), jnp.float32),
            pltpu.SemaphoreType.DMA((len(operands),)),
            pltpu.SemaphoreType.DMA((2,)),
            pltpu.SemaphoreType.DMA((sp_size,)),
            pltpu.SemaphoreType.DMA((sp_size,)),
            pltpu.SemaphoreType.DMA((far_size, steps)),
            pltpu.SemaphoreType.DMA((far_size, steps)),
            pltpu.SemaphoreType.DMA((far_slots, steps)),
            pltpu.SemaphoreType.DMA((far_slots, steps)),
        ],
        compiler_params=pltpu.CompilerParams(
            collective_id=0, has_side_effects=True, vmem_limit_bytes=67043328
        ),
    )(*operands)


def slot_numbers(picks, experts):
    flat = picks.reshape(-1)
    onehot = (flat[:, None] == jnp.arange(experts, dtype=jnp.int32)[None, :]).astype(jnp.int32)
    before = jnp.cumsum(onehot, axis=0) - onehot
    return (flat, jnp.sum(before * onehot, axis=1))


def fill_slots(source_rows, slot_of, row_of, slot_count):
    match = slot_of[None, :] == jnp.arange(slot_count, dtype=jnp.int32)[:, None]
    picked = jnp.sum(jnp.where(match, row_of[None, :], 0), axis=1)
    present = jnp.any(match, axis=1)
    return jnp.where(present[:, None], source_rows[picked], jnp.zeros((), source_rows.dtype))


def expert_hidden(rows, gate_weight, up_weight):
    gate = jnp.dot(rows, gate_weight[0], preferred_element_type=jnp.float32)
    upward = jnp.dot(rows, up_weight[0], preferred_element_type=jnp.float32)
    return (jax.nn.silu(gate) * upward).astype(jnp.bfloat16)


def expert_down(active, down_weight):
    columns = down_weight[0]
    return jnp.dot(
        lax.all_gather(active, "tp", axis=1, tiled=True),
        columns,
        preferred_element_type=jnp.float32,
    ).astype(jnp.bfloat16)


def phase(name):
    return contextlib.nullcontext()


def layer_kernel(
    sp_size,
    tp_size,
    capacity,
    x_hbm,
    out_gate_hbm,
    taps_hbm,
    recur_map_hbm,
    input_map_hbm,
    decay_hbm,
    boost_hbm,
    routes_hbm,
    pair_weight_hbm,
    weight_hbm,
    resid_hbm,
    gain_hbm,
    gate_hbm,
    up_hbm,
    down_hbm,
    out_ref,
    x_ref,
    out_gate_ref,
    taps_ref,
    recur_map_ref,
    input_map_ref,
    decay_ref,
    boost_ref,
    routes_ref,
    pair_weight_ref,
    weight_ref,
    resid_ref,
    gain_ref,
    gate,
    up,
    down,
    gates_ref,
    ext,
    rim,
    running,
    local,
    lifted,
    branch,
    totals,
    across,
    along,
    send_pair,
    recv_pair,
    send_far,
    recv_far,
    summed,
    stream_ref,
    normed_ref,
    other_normed,
    mirrored,
    own_weights,
    pair_weights,
    ranks,
    choose,
    choose_other,
    choose_mirror,
    mixers,
    outgoing,
    outgoing_other,
    outgoing_mirror,
    rows,
    active,
    result,
    returned,
    blend,
    gathered,
    gate_extra,
    up_extra,
    load_sems,
    rim_sems,
    extra_send,
    extra_recv,
    total_send,
    total_recv,
    pair_send,
    pair_recv,
    far_send,
    far_recv,
    cross_send,
    cross_recv,
    mirror_send,
    mirror_recv,
    route_sems,
    weight_send,
    weight_recv,
    out_send,
    out_recv,
    near_send,
    near_recv,
    pass_send,
    pass_recv,
    row_far_send,
    row_far_recv,
    row_pair_send,
    row_pair_recv,
    half_send,
    half_recv,
    half_pair_send,
    half_pair_recv,
    back_half_send,
    back_half_recv,
    blend_send,
    blend_recv,
    store_sems,
):
    sp, tp = lax.axis_index("sp"), lax.axis_index("tp")
    tokens, channels = x_ref.shape
    taps = taps_ref.shape[0]
    rows_dev, width = resid_ref.shape
    picks = routes_ref.shape[1]
    hidden, columns = gate.shape[1], down.shape[1]
    core, far = lax.rem(tp, 2), tp // 2
    other = 1 - far
    partner = far * 2 + 1 - core
    across_tp = other * 2 + core
    half = sp_size // 2
    steps, step = send_pair.shape[1], send_pair.shape[3]
    kept = hidden - gate_extra.shape[1]
    pieces = far_send.shape[0]
    piece = rows_dev // pieces

    def flipped(d):
        total, bit = 0, 1
        while bit < sp_size:
            total = total + bit * lax.rem(sp // bit + d // bit, 2)
            bit *= 2
        return total

    sources = (
        (x_hbm, x_ref),
        (out_gate_hbm, out_gate_ref),
        (taps_hbm, taps_ref),
        (recur_map_hbm, recur_map_ref),
        (input_map_hbm, input_map_ref),
        (decay_hbm, decay_ref),
        (boost_hbm, boost_ref),
        (routes_hbm, routes_ref.at[0:tp_size]),
        (pair_weight_hbm, pair_weight_ref),
        (weight_hbm, weight_ref),
        (resid_hbm, resid_ref),
        (gain_hbm, gain_ref),
        (gate_hbm.at[0], gate),
        (up_hbm.at[0], up),
        (down_hbm.at[0], down),
    )
    loads = [
        pltpu.make_async_copy(source, target, load_sems.at[n])
        for n, (source, target) in enumerate(sources)
    ]
    for load in loads[:12]:
        load.start()

    barrier = pltpu.get_barrier_semaphore()
    for d in range(1, sp_size):
        pl.semaphore_signal(barrier, inc=1, **at_device(lax.rem(sp + d, sp_size), tp))
    for u in range(1, tp_size):
        pl.semaphore_signal(barrier, inc=1, **at_device(sp, lax.rem(tp + u, tp_size)))

    loads[0].wait()
    chunks = tokens // CHUNK

    @pl.loop(0, chunks)
    def _(i):
        r = pl.multiple_of(i * CHUNK, CHUNK)
        ext[pl.ds(r + TILE, CHUNK), :] = x_ref[pl.ds(r, CHUNK), :].astype(jnp.float32)

    for load in loads[2:6]:
        load.wait()
    map_size = recur_map_ref.shape[1]
    per = LANES // map_size
    gates_ref[...] = jnp.zeros_like(gates_ref)
    for b in range(channels // LANES):
        for n in range(per):
            spots = slice(n * map_size, (n + 1) * map_size)
            for side, maps in enumerate((recur_map_ref, input_map_ref)):
                start = side * LANES + n * map_size
                gates_ref[b, spots, start : start + map_size] = maps[b * per + n]
    raw = decay_ref[...]
    small = jnp.exp(-jnp.abs(raw))
    series = small * (1 - small * (1 / 2 - small * (1 / 3 - small * (1 / 4 - small * (1 / 5 - small / 6)))))
    plus = jnp.maximum(-raw, 0.0) + jnp.where(small < 0.05, series, jnp.log(1.0 + small))
    scale = -RECURRENT_SCALE * plus

    loads[8].wait()
    own_weights[...] = jnp.zeros_like(own_weights)
    own_weights[0:picks, :] = pair_weight_ref[...]
    pair_weights[tp] = own_weights[...]

    with phase("barrier"):
        pl.semaphore_wait(barrier, sp_size - 1 + tp_size - 1)
    rim_copy = pltpu.make_async_remote_copy(
        src_ref=x_ref.at[pl.ds(tokens - RIM, RIM)],
        dst_ref=rim,
        send_sem=rim_sems.at[0],
        recv_sem=rim_sems.at[1],
        **at_device(lax.rem(sp + 1, sp_size), tp),
    )
    rim_copy.start()

    def extra_copy(n):
        source, target = ((gate_hbm, gate_extra), (up_hbm, up_extra))[n]
        return pltpu.make_async_remote_copy(
            src_ref=source.at[0, :, kept:hidden],
            dst_ref=target,
            send_sem=extra_send.at[n],
            recv_sem=extra_recv.at[n],
            **at_device(sp, across_tp),
        )

    @pl.when(core == 0)
    def _():
        for n in range(2):
            extra_copy(n).start()

    def weight_copy(u):
        return pltpu.make_async_remote_copy(
            src_ref=own_weights,
            dst_ref=pair_weights.at[tp],
            send_sem=weight_send.at[u],
            recv_sem=weight_recv.at[u],
            **at_device(sp, lax.rem(tp + u, tp_size)),
        )

    for u in range(1, tp_size):
        weight_copy(u).start()
    loads[7].wait()
    route_copy = pltpu.make_async_remote_copy(
        src_ref=routes_ref.at[tp],
        dst_ref=routes_ref.at[tp_size],
        send_sem=route_sems.at[0],
        recv_sem=route_sems.at[1],
        **at_device(flipped(half), tp),
    )
    route_copy.start()
    loads[6].wait()
    for load in loads[12:]:
        load.start()

    tile_row = lax.broadcasted_iota(jnp.int32, (CHUNK, LANES), 0) % TILE

    def chunk(i, carry):
        r = pl.multiple_of(i * CHUNK, CHUNK)
        out = []
        for b in range(channels // LANES):
            cols = slice(b * LANES, (b + 1) * LANES)
            win = ext[pl.ds(r, CHUNK + TILE), cols]
            base = TILE - taps + 1
            mixed = win[base : base + CHUNK] * taps_ref[0:1, cols]
            for k in range(1, taps):
                mixed = mixed + win[base + k : base + k + CHUNK] * taps_ref[k : k + 1, cols]
            smoothed = mixed.astype(jnp.bfloat16)
            both = jnp.dot(smoothed, gates_ref[b], preferred_element_type=jnp.float32)
            recur = jax.nn.sigmoid(both[:, :LANES])
            inward = jax.nn.sigmoid(both[:, LANES:])
            log_decay = recur * scale[0:1, cols] + boost_ref[pl.ds(r, CHUNK), cols]
            a = jnp.exp(log_decay)
            h = jnp.sqrt(one_minus_exp(2.0 * log_decay)) * (inward * smoothed.astype(jnp.float32))
            for s in (1, 2, 4):
                inside = tile_row >= s
                a_before = jnp.where(inside, pltpu.roll(a, s, 0), 1.0)
                h_before = jnp.where(inside, pltpu.roll(h, s, 0), 0.0)
                h = a * h_before + h
                a = a * a_before
            carry_a, carry_h = carry[2 * b], carry[2 * b + 1]
            for t in range(CHUNK // TILE):
                spots = slice(t * TILE, (t + 1) * TILE)
                h_t = h[spots] + a[spots] * carry_h
                a_t = a[spots] * carry_a
                running[pl.ds(r + t * TILE, TILE), cols] = a_t
                local[pl.ds(r + t * TILE, TILE), cols] = h_t
                carry_a, carry_h = a_t[TILE - 1 : TILE], h_t[TILE - 1 : TILE]
            out += [carry_a, carry_h]
        return tuple(out)

    ones, zeros = jnp.ones((1, LANES), jnp.float32), jnp.zeros((1, LANES), jnp.float32)
    start = (ones, zeros) * (channels // LANES)
    with phase("scan"):
        rest = lax.fori_loop(1, chunks, chunk, start)
    with phase("rim"):
        rim_copy.wait()
    edge = rim[...].astype(jnp.float32)[RIM - TILE :, :]
    ext[0:TILE, :] = jnp.where(sp == 0, 0.0, edge)
    with phase("head"):
        first = lax.fori_loop(0, 1, chunk, start)
    pick = lax.broadcasted_iota(jnp.int32, (TILE, LANES), 0) == 0
    for b in range(channels // LANES):
        first_a, first_h, rest_a, rest_h = first[2 * b], first[2 * b + 1], rest[2 * b], rest[2 * b + 1]
        totals[sp, :, b * LANES : (b + 1) * LANES] = jnp.where(
            pick, first_a * rest_a, rest_a * first_h + rest_h
        )
    head_a = jnp.concatenate(first[0::2], axis=1)
    head_h = jnp.concatenate(first[1::2], axis=1)

    total_copies = []
    for d in range(1, sp_size):
        copy = pltpu.make_async_remote_copy(
            src_ref=totals.at[sp],
            dst_ref=totals.at[sp],
            send_sem=total_send.at[d],
            recv_sem=total_recv.at[d],
            **at_device(lax.rem(sp + d, sp_size), tp),
        )
        copy.start()
        total_copies.append(copy)

    loads[1].wait()

    with phase("gelu"):

        @pl.loop(0, chunks)
        def _(i):
            r = pl.multiple_of(i * CHUNK, CHUNK)
            lifted[pl.ds(r, CHUNK), :] = jax.nn.gelu(
                out_gate_ref[pl.ds(r, CHUNK), :].astype(jnp.float32)
            )

    for load in loads[9:12]:
        load.wait()
    with phase("totals"):
        for copy in total_copies:
            copy.wait()

    entering = jnp.zeros((1, channels), jnp.float32)
    for k in range(sp_size):
        part = totals[k]
        after = part[0:1] * entering + part[1:2]
        entering = jnp.where(k < sp, after, entering)
    entering_rest = head_a * entering + head_h

    both_rows = 2 * rows_dev

    def fill_branch(side):
        for q in range(both_rows // CHUNK):
            r = pl.multiple_of(side * both_rows + q * CHUNK, CHUNK)
            at = pl.ds(r, CHUNK)
            before = entering_rest
            if q == 0:
                before = jnp.where(side == 0, entering, entering_rest)
            state = local[at, :] + running[at, :] * before
            branch[at, :] = (lifted[at, :] * state).astype(jnp.bfloat16)

    def pair_copy(k, n):
        return pltpu.make_async_remote_copy(
            src_ref=send_pair.at[k, n],
            dst_ref=recv_pair.at[k, n],
            send_sem=pair_send.at[k, n],
            recv_sem=pair_recv.at[k, n],
            **at_device(sp, partner),
        )

    def project(side, target, k, send):
        fill_branch(side)
        given = branch[pl.ds(pl.multiple_of(side * both_rows, both_rows), both_rows), :]
        for n in range(steps):
            cols = slice(n * step, (n + 1) * step)
            product = jnp.dot(given, weight_ref[:, cols], preferred_element_type=jnp.float32)
            target[0, :, cols] = product[:rows_dev]
            target[1, :, cols] = product[rows_dev:]
            send_pair[k, n] = target[1 - core, :, cols].astype(jnp.bfloat16)
            if send:
                pair_copy(k, n).start()

    with phase("project"):
        project(other, across, 0, True)

    def far_copy(q):
        return pltpu.make_async_remote_copy(
            src_ref=send_far.at[pl.ds(q * piece, piece)],
            dst_ref=recv_far.at[pl.ds(q * piece, piece)],
            send_sem=far_send.at[q],
            recv_sem=far_recv.at[q],
            **at_device(sp, across_tp),
        )

    with phase("far_send"):
        for n in range(steps):
            pair_copy(0, n).wait_recv()
        for q in range(pieces):
            at = slice(q * piece, (q + 1) * piece)
            for n in range(steps):
                cols = slice(n * step, (n + 1) * step)
                sum_far = across[core, at, cols] + recv_pair[0, n, at, :].astype(jnp.float32)
                send_far[at, cols] = sum_far.astype(jnp.bfloat16)
            far_copy(q).start()
    project(far, along, 1, True)
    for n in range(steps):
        cols = slice(n * step, (n + 1) * step)
        pair_copy(1, n).wait_recv()
        summed[:, cols] = (
            along[core, :, cols]
            + resid_ref[:, cols].astype(jnp.float32)
            + recv_pair[1, n].astype(jnp.float32)
        )

    slot_row = lax.broadcasted_iota(jnp.int32, (capacity, rows_dev), 0)
    expert_row = lax.broadcasted_iota(jnp.int32, (sp_size, rows_dev), 0)
    earlier = lax.broadcasted_iota(jnp.int32, (rows_dev, rows_dev), 0) < lax.broadcasted_iota(
        jnp.int32, (rows_dev, rows_dev), 1
    )
    earlier = jnp.where(earlier, 1.0, 0.0).astype(jnp.bfloat16)

    route_copy.wait()

    @pl.loop(0, tp_size + 1)
    def _(block):
        chosen = routes_ref[block]
        hits = jnp.zeros((sp_size, rows_dev), jnp.float32)
        for k in range(picks):
            hits = hits + jnp.where(expert_row == chosen[k : k + 1], 1.0, 0.0)
        ranks[block] = jnp.dot(hits.astype(jnp.bfloat16), earlier, preferred_element_type=jnp.float32)

    def selector(block, expert, values):
        chosen = routes_ref[block]
        value = jnp.zeros((1, rows_dev), jnp.float32)
        for k in range(picks):
            value = value + jnp.where(chosen[k : k + 1] == expert, values[k : k + 1], 0.0)
        rank = ranks[block, pl.ds(expert, 1), :].astype(jnp.int32)
        return jnp.where(rank == slot_row, value, 0.0)

    def slot_rows(block):
        return pl.ds(pl.multiple_of(block * capacity, capacity), capacity)

    unit = jnp.ones((picks, rows_dev), jnp.float32)

    @pl.loop(0, half)
    def _(d):
        expert = flipped(d)
        choose[slot_rows(d), :] = selector(tp, expert, unit).astype(jnp.bfloat16)
        choose_other[slot_rows(d), :] = selector(across_tp, expert, unit).astype(jnp.bfloat16)
        choose_mirror[slot_rows(d), :] = selector(tp_size, expert, unit).astype(jnp.bfloat16)

    with phase("weights"):
        for u in range(1, tp_size):
            weight_copy(u).wait_recv()

    with phase("mixers"):

        @pl.loop(0, tp_size)
        def _(block):
            weight = pair_weights[block]
            coarse = weight.astype(jnp.bfloat16).astype(jnp.float32)
            for n, values in enumerate((coarse, weight - coarse)):
                picked = [selector(block, e, values) for e in range(sp_size)]
                mixers[block, n] = jnp.concatenate(picked, axis=0).T.astype(jnp.bfloat16)

    def cross_copy(q):
        return pltpu.make_async_remote_copy(
            src_ref=normed_ref.at[pl.ds(q * piece, piece)],
            dst_ref=other_normed.at[pl.ds(q * piece, piece)],
            send_sem=cross_send.at[q],
            recv_sem=cross_recv.at[q],
            **at_device(sp, across_tp),
        )

    def mirror_copy(q):
        return pltpu.make_async_remote_copy(
            src_ref=normed_ref.at[pl.ds(q * piece, piece)],
            dst_ref=mirrored.at[pl.ds(q * piece, piece)],
            send_sem=mirror_send.at[q],
            recv_sem=mirror_recv.at[q],
            **at_device(flipped(half), tp),
        )

    with phase("norm"):
        for q in range(pieces):
            at = slice(q * piece, (q + 1) * piece)
            far_copy(q).wait_recv()
            squares = jnp.zeros((piece, 1), jnp.float32)
            for n in range(steps):
                cols = slice(n * step, (n + 1) * step)
                stream = (summed[at, cols] + recv_far[at, cols].astype(jnp.float32)).astype(jnp.bfloat16)
                stream_ref[at, cols] = stream
                wide = stream.astype(jnp.float32)
                squares = squares + jnp.sum(wide * wide, axis=1, keepdims=True)
            norm = lax.rsqrt(squares * (1.0 / width) + EPSILON)
            for n in range(steps):
                cols = slice(n * step, (n + 1) * step)
                wide = stream_ref[at, cols].astype(jnp.float32)
                normed_ref[at, cols] = (wide * norm * gain_ref[0:1, cols]).astype(jnp.bfloat16)
            cross_copy(q).start()
            mirror_copy(q).start()

    def out_copy(d):
        return pltpu.make_async_remote_copy(
            src_ref=outgoing.at[slot_rows(d)],
            dst_ref=rows.at[sp, slot_rows(tp)],
            send_sem=out_send.at[d],
            recv_sem=out_recv.at[d],
            **at_device(flipped(d), tp),
        )

    def near_copy(d):
        return pltpu.make_async_remote_copy(
            src_ref=outgoing_other.at[slot_rows(d)],
            dst_ref=rows.at[sp, slot_rows(across_tp)],
            send_sem=near_send.at[d],
            recv_sem=near_recv.at[d],
            **at_device(flipped(d), tp),
        )

    def pass_copy(e):
        return pltpu.make_async_remote_copy(
            src_ref=outgoing_mirror.at[slot_rows(e)],
            dst_ref=rows.at[flipped(half), slot_rows(tp)],
            send_sem=pass_send.at[e],
            recv_sem=pass_recv.at[e],
            **at_device(flipped(e), tp),
        )

    def row_far(d):
        place = rows.at[flipped(d), slot_rows(tp)]
        return pltpu.make_async_remote_copy(
            src_ref=place,
            dst_ref=place,
            send_sem=row_far_send.at[d - half],
            recv_sem=row_far_recv.at[d - half],
            **at_device(sp, across_tp),
        )

    def row_pair(d, j):
        place = rows.at[flipped(d), slot_rows(across_tp if j else tp)]
        return pltpu.make_async_remote_copy(
            src_ref=place,
            dst_ref=place,
            send_sem=row_pair_send.at[d, j],
            recv_sem=row_pair_recv.at[d, j],
            **at_device(sp, partner),
        )

    half_slots = 2 * capacity

    def side_rows(side):
        return pl.ds(pl.multiple_of(side * half_slots, half_slots), half_slots)

    sides = (far, other)

    def half_copy(d, h, end):
        place = active.at[flipped(d), tp, side_rows(sides[h]), 0:end]
        return pltpu.make_async_remote_copy(
            src_ref=place,
            dst_ref=place,
            send_sem=half_send.at[d, h],
            recv_sem=half_recv.at[d, h],
            **at_device(sp, across_tp),
        )

    def on_half(d, h, act):
        @pl.when(core == 0)
        def _():
            act(half_copy(d, h, kept))

        @pl.when(core == 1)
        def _():
            act(half_copy(d, h, hidden))

    def half_start(d, h):
        on_half(d, h, lambda copy: copy.start())

    def half_pair(d, j, h):
        place = active.at[flipped(d), across_tp if j else tp, side_rows(sides[h])]
        return pltpu.make_async_remote_copy(
            src_ref=place,
            dst_ref=place,
            send_sem=half_pair_send.at[d, 2 * j + h],
            recv_sem=half_pair_recv.at[d, 2 * j + h],
            **at_device(sp, partner),
        )

    def back_half(d, h):
        return pltpu.make_async_remote_copy(
            src_ref=result.at[d, side_rows(sides[h])],
            dst_ref=returned.at[sp, side_rows(sides[h])],
            send_sem=back_half_send.at[d, h],
            recv_sem=back_half_recv.at[d, h],
            **at_device(flipped(d), tp),
        )

    mates = (across_tp, other * 2 + 1 - core, partner)

    def blend_copy(u):
        return pltpu.make_async_remote_copy(
            src_ref=blend.at[u],
            dst_ref=gathered.at[tp],
            send_sem=blend_send.at[u],
            recv_sem=blend_recv.at[u],
            **at_device(sp, mates[u]),
        )

    pack_rows = half * capacity

    def pack(chooser, given, target):
        for n in range(steps):
            cols = slice(n * step, (n + 1) * step)
            target[:, cols] = jnp.dot(
                chooser[...], given[:, cols], preferred_element_type=jnp.float32
            ).astype(jnp.bfloat16)

    def hidden_part(given, gate_part, up_part):
        gated = jnp.dot(given, gate_part[...], preferred_element_type=jnp.float32)
        upward = jnp.dot(given, up_part[...], preferred_element_type=jnp.float32)
        return (jax.nn.silu(gated) * upward).astype(jnp.bfloat16)

    def fill_hidden(d, h):
        source = flipped(d)
        at = side_rows(sides[h])
        active[source, tp, at, :] = hidden_part(rows[source, at, :], gate, up)
        half_pair(d, 0, h).start()

    def fill_extra(d, h):
        source = flipped(d)
        at = side_rows(sides[h])

        @pl.when(core == 0)
        def _():
            active[source, across_tp, at, kept:hidden] = hidden_part(
                rows[source, at, :], gate_extra, up_extra
            )

    def first(d):
        with phase("w_first"):
            row_pair(d, 0).wait_recv()
        fill_hidden(d, 0)
        half_start(d, 0)
        fill_extra(d, 0)

    def second(d):
        with phase("w_second"):
            row_pair(d, 1).wait_recv()
        fill_hidden(d, 1)
        fill_extra(d, 1)

    def relay(d, h):
        with phase("w_relay"):
            on_half(d, h, lambda copy: copy.wait_recv())
        half_pair(d, 1, 1 - h).start()

    def down_side(d, h):
        with phase("w_down"):
            half_pair(d, 0, h).wait_recv()
            half_pair(d, 1, h).wait_recv()
        source = flipped(d)
        at = side_rows(sides[h])
        total = jnp.dot(active[source, 0, at, :], down[0:hidden, :], preferred_element_type=jnp.float32)
        for t in range(1, tp_size):
            total = total + jnp.dot(
                active[source, t, at, :],
                down[t * hidden : (t + 1) * hidden, :],
                preferred_element_type=jnp.float32,
            )
        made = total.astype(jnp.bfloat16)
        result[d, at, :] = made

        @pl.when(d == 0)
        def _():
            returned[sp, at, :] = made

        @pl.when(d > 0)
        def _():
            back_half(d, h).start()

    def near_first(d):
        with phase("w_own"):

            @pl.when(d > 0)
            def _():
                out_copy(d).wait_recv()
                row_pair(d, 0).start()

        first(d)

    def near_arrived(d):
        with phase("w_near"):

            @pl.when(d > 0)
            def _():
                near_copy(d).wait_recv()
                row_pair(d, 1).start()

    with phase("pack"):
        pack(choose, normed_ref, outgoing)
        out_copy(1).start()
        rows[sp, slot_rows(tp), :] = outgoing[0:capacity, :]
        row_pair(0, 0).start()
    for load in loads[12:]:
        load.wait()

    @pl.when(core == 0)
    def _():
        for n in range(2):
            extra_copy(n).wait_recv()

    @pl.loop(0, half // 2)
    def _(d):
        near_first(d)

    with phase("cross"):
        for q in range(pieces):
            cross_copy(q).wait_recv()
    with phase("pack_other"):
        pack(choose_other, other_normed, outgoing_other)
        rows[sp, slot_rows(across_tp), :] = outgoing_other[0:capacity, :]
        row_pair(0, 1).start()
    with phase("mirror"):
        for q in range(pieces):
            mirror_copy(q).wait_recv()
    with phase("pack_mirror"):
        pack(choose_mirror, mirrored, outgoing_mirror)
        for e in range(1, min(3, half)):
            pass_copy(e).start()
        near_copy(1).start()
        rows[flipped(half), slot_rows(tp), :] = outgoing_mirror[0:capacity, :]
        row_far(half).start()
        row_pair(half, 0).start()

    first(half)

    @pl.loop(1, half + 1)
    def _(s):
        d = half + s
        near = s - 1

        @pl.when(s < half)
        def _():
            with phase("w_pass"):
                pass_copy(s).wait_recv()
            row_far(d).start()
            row_pair(d, 0).start()

        @pl.when(s + 2 < half)
        def _():
            pass_copy(s + 2).start()

        @pl.when(s + 1 < half)
        def _():
            out_copy(s + 1).start()
            near_copy(s + 1).start()

        with phase("w_rowfar"):
            row_far(d - 1).wait_recv()
        row_pair(d - 1, 1).start()

        @pl.when(s >= 2)
        def _():
            relay(d - 2, 1)

        @pl.when(s < half)
        def _():
            first(d)

        second(d - 1)
        half_start(d - 1, 1)
        relay(d - 1, 0)
        near_arrived(near)

        @pl.when(s >= 2)
        def _():
            down_side(d - 2, 0)

        @pl.when(near >= half // 2)
        def _():
            near_first(near)

        down_side(d - 1, 1)

        second(near)

        @pl.when(near < half // 2)
        def _():
            relay(near, 0)
            down_side(near, 1)

    for d in reversed(range(half)):
        half_start(d, 1)

    relay(sp_size - 1, 1)

    @pl.loop(half // 2, half)
    def _(d):
        relay(d, 0)
        down_side(d, 1)

    down_side(sp_size - 1, 0)

    @pl.loop(1, half)
    def _(d):
        relay(half - d, 1)

    @pl.loop(1, half)
    def _(d):
        down_side(half - d, 0)

    def blended(block):
        part = returned[:, slot_rows(block), :].reshape(sp_size * capacity, columns)
        total = jnp.dot(mixers[block, 0], part, preferred_element_type=jnp.float32)
        total = total + jnp.dot(mixers[block, 1], part, preferred_element_type=jnp.float32)
        return total.astype(jnp.bfloat16)

    with phase("w_back"):

        @pl.loop(1, sp_size)
        def _(d):
            back_half(d, 1).wait_recv()

    with phase("blend"):
        for u in range(2):
            blend[u] = blended(mates[u])
            blend_copy(u).start()

    relay(0, 1)
    down_side(0, 0)

    @pl.loop(1, sp_size)
    def _(d):
        back_half(d, 0).wait_recv()

    blend[2] = blended(partner)
    blend_copy(2).start()
    gathered[tp] = blended(tp)
    def finish(n, t):
        cols = pl.ds(pl.multiple_of(t * columns, columns), columns)
        normed_ref[:, cols] = (
            stream_ref[:, cols].astype(jnp.float32) + gathered[t].astype(jnp.float32)
        ).astype(jnp.bfloat16)
        pltpu.make_async_copy(normed_ref.at[:, cols], out_ref.at[:, cols], store_sems.at[n]).start()

    for k in range(2):
        for n in range(steps):
            pair_copy(k, n).wait_send()
    for q in range(pieces):
        far_copy(q).wait_send()
        cross_copy(q).wait_send()
        mirror_copy(q).wait_send()
    for u in range(1, tp_size):
        weight_copy(u).wait_send()

    @pl.when(core == 0)
    def _():
        for n in range(2):
            extra_copy(n).wait_send()


    @pl.loop(1, half)
    def _(d):
        out_copy(d).wait_send()
        near_copy(d).wait_send()
        pass_copy(d).wait_send()

    @pl.loop(1, sp_size)
    def _(d):
        for h in range(2):
            back_half(d, h).wait_send()

    @pl.loop(half, sp_size)
    def _(d):
        row_far(d).wait_send()

    @pl.loop(0, sp_size)
    def _(d):
        for h in range(2):
            row_pair(d, h).wait_send()
            on_half(d, h, lambda copy: copy.wait_send())
            for j in range(2):
                half_pair(d, j, h).wait_send()

    finish(0, tp)
    for n, u in enumerate((2, 0, 1)):
        with phase("w_blend"):
            blend_copy(u).wait_recv()
        finish(n + 1, mates[u])
    for u in range(tp_size - 1):
        blend_copy(u).wait_send()
    for n, t in enumerate((tp, mates[2], mates[0], mates[1])):
        cols = pl.ds(pl.multiple_of(t * columns, columns), columns)
        pltpu.make_async_copy(normed_ref.at[:, cols], out_ref.at[:, cols], store_sems.at[n]).wait()


def fused_layer(
    resid,
    recurrent_input,
    recurrent_out_gate,
    filter_weight,
    recurrence_gate_matrix,
    input_gate_matrix,
    channel_decay_raw,
    token_decay_boost,
    output_projection_weight,
    expert_norm_gain,
    routes,
    expert_pair_weight,
    gate_weight,
    up_weight,
    down_weight,
    capacity,
):
    sp_size, tp_size = lax.axis_size("sp"), lax.axis_size("tp")
    tokens, channels = recurrent_input.shape
    rows_dev, width = resid.shape
    hidden, columns = gate_weight.shape[2], down_weight.shape[2]
    step = 512 if width % 512 == 0 else width
    steps = width // step
    pieces = 8 if rows_dev % (8 * RIM) == 0 else 1
    half = sp_size // 2
    slots_all = tp_size * capacity
    narrow = (
        recurrent_input,
        recurrent_out_gate,
        filter_weight,
        recurrence_gate_matrix,
        input_gate_matrix,
        channel_decay_raw.reshape(1, channels),
        token_decay_boost,
        routes.reshape(tp_size, rows_dev, -1).swapaxes(1, 2),
        expert_pair_weight.T,
        output_projection_weight,
        resid,
        expert_norm_gain.reshape(1, width),
    )
    operands = (*narrow, gate_weight, up_weight, down_weight)
    dma = pltpu.SemaphoreType.DMA

    def buffer(*shape):
        return pltpu.VMEM(shape, jnp.bfloat16)

    def wide(*shape):
        return pltpu.VMEM(shape, jnp.float32)

    return pl.pallas_call(
        functools.partial(layer_kernel, sp_size, tp_size, capacity),
        out_shape=jax.ShapeDtypeStruct((rows_dev, width), jnp.bfloat16),
        in_specs=[pl.BlockSpec(memory_space=pltpu.HBM)] * len(operands),
        out_specs=pl.BlockSpec(memory_space=pltpu.HBM),
        scratch_shapes=[
            *[pltpu.VMEM(operand.shape, operand.dtype) for operand in narrow[:7]],
            pltpu.VMEM((tp_size + 1, *narrow[7].shape[1:]), narrow[7].dtype),
            *[pltpu.VMEM(operand.shape, operand.dtype) for operand in narrow[8:]],
            buffer(*gate_weight.shape[1:]),
            buffer(*up_weight.shape[1:]),
            buffer(*down_weight.shape[1:]),
            buffer(channels // LANES, LANES, 2 * LANES),
            wide(tokens + TILE, channels),
            buffer(RIM, channels),
            wide(tokens, channels),
            wide(tokens, channels),
            wide(tokens, channels),
            buffer(tokens, channels),
            wide(sp_size, TILE, channels),
            wide(2, rows_dev, width),
            wide(2, rows_dev, width),
            buffer(2, steps, rows_dev, step),
            buffer(2, steps, rows_dev, step),
            buffer(rows_dev, width),
            buffer(rows_dev, width),
            wide(rows_dev, width),
            buffer(rows_dev, width),
            buffer(rows_dev, width),
            buffer(rows_dev, width),
            buffer(rows_dev, width),
            wide(TILE, rows_dev),
            wide(tp_size, TILE, rows_dev),
            wide(tp_size + 1, sp_size, rows_dev),
            *[buffer(half * capacity, rows_dev)] * 3,
            buffer(tp_size, 2, rows_dev, sp_size * capacity),
            *[buffer(half * capacity, width)] * 3,
            buffer(sp_size, slots_all, width),
            buffer(sp_size, tp_size, slots_all, hidden),
            buffer(sp_size, slots_all, columns),
            buffer(sp_size, slots_all, columns),
            buffer(tp_size - 1, rows_dev, columns),
            buffer(tp_size, rows_dev, columns),
            buffer(width, LANES),
            buffer(width, LANES),
            dma((len(operands),)),
            dma((2,)),
            dma((2,)),
            dma((2,)),
            dma((sp_size,)),
            dma((sp_size,)),
            dma((2, steps)),
            dma((2, steps)),
            *[dma((pieces,))] * 6,
            dma((2,)),
            dma((tp_size,)),
            dma((tp_size,)),
            *[dma((half,))] * 8,
            *[dma((sp_size, 2))] * 4,
            dma((sp_size, 4)),
            dma((sp_size, 4)),
            dma((sp_size, 2)),
            dma((sp_size, 2)),
            dma((tp_size - 1,)),
            dma((tp_size - 1,)),
            dma((tp_size,)),
        ],
        compiler_params=pltpu.CompilerParams(
            collective_id=1, has_side_effects=True, vmem_limit_bytes=58720256
        ),
    )(*operands)


def body(
    resid,
    recurrent_input,
    recurrent_out_gate,
    filter_weight,
    recurrence_gate_matrix,
    input_gate_matrix,
    channel_decay_raw,
    token_decay_boost,
    output_projection_weight,
    expert_norm_gain,
    routes,
    expert_pair_weight,
    gate_weight,
    up_weight,
    down_weight,
):
    tp_size = lax.axis_size("tp")
    experts = lax.axis_size("sp")
    rows_dev, model_width = resid.shape
    capacity = max(2, 3 * rows_dev // experts)
    fits = capacity % RIM == 0 and rows_dev % LANES == 0
    fits = fits and gate_weight.shape[2] % LANES == 0 and gate_weight.shape[2] > LANES
    if fits and tp_size == 4 and experts >= 4 and experts & (experts - 1) == 0:
        return fused_layer(
            resid,
            recurrent_input,
            recurrent_out_gate,
            filter_weight,
            recurrence_gate_matrix,
            input_gate_matrix,
            channel_decay_raw,
            token_decay_boost,
            output_projection_weight,
            expert_norm_gain,
            routes,
            expert_pair_weight,
            gate_weight,
            up_weight,
            down_weight,
            capacity,
        )
    stream, normed = recurrence(
        resid,
        recurrent_input,
        recurrent_out_gate,
        filter_weight,
        recurrence_gate_matrix,
        input_gate_matrix,
        channel_decay_raw,
        token_decay_boost,
        output_projection_weight,
        expert_norm_gain,
    )
    stream_wide = stream.astype(jnp.float32)
    own_routes = lax.dynamic_slice_in_dim(routes, lax.axis_index("tp") * rows_dev, rows_dev, 0)
    own_flat, own_rank = slot_numbers(own_routes, experts)
    own_slots = own_flat * capacity + own_rank
    row_of = jnp.arange(2 * rows_dev, dtype=jnp.int32) // 2
    outgoing = fill_slots(normed, own_slots, row_of, experts * capacity).reshape(
        experts, capacity, model_width
    )
    arrived = lax.all_to_all(outgoing, "sp", split_axis=0, concat_axis=0, tiled=True)
    piece = lax.all_gather(
        arrived.reshape(1, experts * capacity, model_width), "tp", axis=0, tiled=True
    )
    flat_rows = piece.reshape(piece.shape[0] * piece.shape[1], model_width)
    active = expert_hidden(flat_rows, gate_weight, up_weight).reshape(
        piece.shape[0], piece.shape[1], -1
    )
    result = expert_down(active.reshape(-1, active.shape[2]), down_weight)
    joined = lax.all_to_all(
        result.reshape(tp_size, experts * capacity, -1),
        "tp",
        split_axis=0,
        concat_axis=2,
        tiled=True,
    )
    returned = lax.all_to_all(
        joined.reshape(experts, capacity, model_width),
        "sp",
        split_axis=0,
        concat_axis=0,
        tiled=True,
    )
    picked = (
        returned.reshape(experts * capacity, model_width)[own_slots]
        .astype(jnp.float32)
        .reshape(rows_dev, 2, model_width)
    )
    blended = jnp.sum(picked * expert_pair_weight[:, :, None], axis=1)
    return (stream_wide + blended).astype(jnp.bfloat16)


def solution(mesh):
    placed = (
        P(("sp", "tp"), None),
        P("sp", "tp"),
        P("sp", "tp"),
        P(None, "tp"),
        P("tp", None, None),
        P("tp", None, None),
        P("tp"),
        P("sp", "tp"),
        P("tp", None),
        P(),
        P("sp", None),
        P(("sp", "tp"), None),
        P("sp", None, "tp"),
        P("sp", None, "tp"),
        P("sp", None, "tp"),
    )
    return jax.shard_map(
        body, mesh=mesh, in_specs=placed, out_specs=P(("sp", "tp"), None), check_vma=False
    )
```
